32 devices in a mesh: sp: 4 (over y, x), tp: 8 (over z, core).
Axes of the slice: x: 2, y: 2, z: 4, core: 2. Of those that a mesh axis runs over, the one named last changes fastest.
Arguments:
- cotangent: bfloat16 [1024, 2048], P('sp', 'tp'), may hold values from -6 to 6
- block_input: bfloat16 [1024, 2048], P('sp', 'tp'), may hold values from -6 to 6
- routes: int32 [1024, 2], P('sp'), may hold values from 0 to 3, all different within a row; in each aligned block of 256 rows (0 to 255, 256 to 511, ...) at most 160 rows name the same one
- route_weights: float32 [1024, 2], P('sp'), may hold values from 0.1 to 0.9
- gate_weight: bfloat16 [4, 2048, 7168], P('sp', None, 'tp'), may hold values from -0.125 to 0.125
- up_weight: bfloat16 [4, 2048, 7168], P('sp', None, 'tp'), may hold values from -0.125 to 0.125
- down_weight: bfloat16 [4, 7168, 2048], P('sp', 'tp'), may hold values from -0.0625 to 0.0625
- out_weight: bfloat16 [1024, 2048], P('tp'), may hold values from -0.1875 to 0.1875
- conv_out: bfloat16 [1024, 1024], P('tp', 'sp'), may hold values from -6 to 6
- gate_pre: bfloat16 [1024, 1024], P('tp', 'sp'), may hold values from -6 to 6
- prior_states: bfloat16 [1024, 1024], P('tp', 'sp'), may hold values from -6 to 6
- recur_weight: bfloat16 [16, 64, 64], replicated, may hold values from -0.75 to 0.75
- input_gate_matrix: bfloat16 [16, 64, 64], replicated, may hold values from -0.75 to 0.75
- decay_param: float32 [1024], replicated, may hold values from 4 to 16
- decay_jump: float32 [1024, 1024], P('tp', 'sp'), may hold values from -1 to 0, as said below
Outputs:
- gate_weight_grad: bfloat16 [4, 2048, 7168], P('sp', None, 'tp')
- up_weight_grad: bfloat16 [4, 2048, 7168], P('sp', None, 'tp')
- down_weight_grad: bfloat16 [4, 7168, 2048], P('sp', 'tp')
- out_weight_grad: float32 [1024, 2048], P('tp', 'sp')
- conv_grad: bfloat16 [1024, 1024], P('tp', 'sp')
- valve_logit_derivative: bfloat16 [1024, 1024], P('tp', 'sp')
The draws below stay inside these ranges and needn't reach their ends.
Inputs may be any that keep to these rules, and one draw needn't show every extreme that they name: In each aligned block of 256 rows (the rows of one index of sp) no expert is named by more than 160 routes, a bound that some block reaches; a row names 2 different experts. `decay_jump`: every entry is at most -1 / 20480.
All inputs are finite; a program needn't handle non-finite values.
Results may differ from the reference program's by a relative error of at most 0.018.
Values may be sent and summed in bfloat16 or wider, within the bound.
A program may use at most 128 MiB of HBM per device.

```python
import math
import jax
import jax.numpy as jnp
import numpy as np
from jax import lax

D = 2048
HEAD_DIM = 64
HEADS = 16
FF = 7168
TOP_K = 2
TOK_DEV = 256
WIDTH = 1024
EXPERTS = 4
TOKENS = 1024
CAP = 160
N_SP = 4
N_TP = 8


def draw_decay_param(key, part):
    keys = jax.random.split(jax.random.fold_in(key, 11), 3)
    share = 0.5
    fast = jax.random.uniform(keys[0], (WIDTH,), jnp.float32) < share
    fast_rate = jnp.exp(jax.random.uniform(keys[1], (WIDTH,), jnp.float32, jnp.log(1.0 / 400.0), jnp.log(1.0 / 100.0)))
    slow_rate = jnp.exp(jax.random.uniform(keys[2], (WIDTH,), jnp.float32, jnp.log(0.1), jnp.log(0.8))) / (8.0 * TOKENS)
    rate = jnp.where(fast, fast_rate, slow_rate)
    return (-jnp.log(jnp.expm1(rate))).astype(jnp.float32)


def draw_decay_jump(key, part):
    keys = jax.random.split(jax.random.fold_in(key, 23), 3)
    blocks = TOKENS // TOK_DEV
    block_rate = jnp.exp(jax.random.uniform(keys[0], (WIDTH, blocks), jnp.float32, jnp.log(0.05), jnp.log(0.4))) / TOKENS
    settled_regime = jnp.repeat(block_rate, TOK_DEV, axis=1)
    deposit_items = jax.random.randint(keys[1], (2,), 0, TOKENS)
    objective_numbers = jnp.log(jax.random.uniform(keys[2], (WIDTH, 2), jnp.float32, 0.6, 0.8))
    sequence_indices = jnp.arange(TOKENS)[None, :]
    clustered_bundles = jnp.where(sequence_indices == deposit_items[0], objective_numbers[:, 0:1], 0.0) + jnp.where(sequence_indices == deposit_items[1], objective_numbers[:, 1:2], 0.0)
    return (clustered_bundles - settled_regime).astype(jnp.float32)


def spiked(array, stream_key, source, target, blocks, factor):
    def block_of(axis_at):
        return (jnp.arange(array.shape[axis_at]) // (array.shape[axis_at] // blocks)).reshape((-1,) + (1,) * (array.ndim - 1 - axis_at))

    first = jax.random.permutation(stream_key, blocks)[block_of(target)]
    far = (block_of(target) + blocks // 2) % blocks
    return jnp.where((block_of(source) == first) | (block_of(source) == far), factor * array, array)


def steps_of(own_key, dims, cuts, smallest, top_value):
    def one(dim, blocks):
        steps = jax.random.uniform(jax.random.fold_in(jax.random.fold_in(own_key, 6), dim), (blocks,), jnp.float32, smallest / len(cuts), top_value / len(cuts))
        return jnp.repeat(jnp.exp(steps), dims[dim] // blocks).reshape((-1,) + (1,) * (len(dims) - dim - 1))

    factor_of = one(*cuts[0])
    for cut in cuts[1:]:
        factor_of = factor_of * one(*cut)
    return factor_of


def routed_block(own_key, own, number, rows, amount, top, limit, lean):
    order = jax.random.permutation(own_key, amount)
    packed, usual = portions_of(amount, rows * top, limit, lean, True), portions_of(amount, rows * top, limit, lean, False)
    places = jnp.arange(amount)

    def named(lengths, turn):
        used = int((lengths > 0).sum())
        fixed = max(1, used // 4)
        passed = fixed + (places - fixed + turn * (used - fixed)) % max(1, amount - fixed)
        return jnp.zeros((amount,), jnp.int32).at[order[jnp.where(places < fixed, places, passed)]].set(jnp.asarray(lengths, jnp.int32))

    lengths = jnp.where(number % 4 == 0, named(packed, number // 4), named(usual, number - number // 4 - 1))
    mixed = jax.random.permutation(jax.random.fold_in(own, 3), amount)
    donor, taker = mixed[0:amount // 2 * 2:2], mixed[1:amount // 2 * 2:2]
    room = jnp.minimum(lengths[donor] - 1, limit - lengths[taker]) // 2
    room = jnp.where((donor == order[0]) | (taker == order[0]) | (lengths[taker] == 0), 0, jnp.maximum(room, 0))
    passed = jax.random.randint(jax.random.fold_in(own, 4), (amount // 2,), 0, 1 << 20) % (room + 1)
    lengths = lengths.at[donor].add(-passed).at[taker].add(passed)
    items = jnp.searchsorted(jnp.cumsum(lengths), jnp.arange(rows * top), side="right").astype(jnp.int32)
    listing = items.reshape(top, rows).T
    listing = listing[jax.random.permutation(jax.random.fold_in(own, 1), rows)]
    turn = jax.random.randint(jax.random.fold_in(own, 2), (rows, 1), 0, top)
    return jnp.take_along_axis(listing, (jnp.arange(top)[None, :] + turn) % top, axis=1)


def portions_of(amount, total, reach, lean, full):
    loads = [(1 << 20) // math.isqrt(standing ** lean) + 1 for standing in range(1, amount + 1)]
    largest = reach if full else min(reach, max(-(-total // amount), total * loads[0] // sum(loads)))
    least = 1 if total - largest >= amount - 1 else 0
    given, rest = [largest] + [least] * (amount - 1), total - largest - least * (amount - 1)
    while rest > 0:
        free = [i for i in range(1, amount) if given[i] < largest] or [i for i in range(1, amount) if given[i] < reach]
        whole, budget = sum([loads[i] for i in free]), rest
        for i in free:
            extra = min(reach - given[i], max(1, budget * loads[i] // whole), rest)
            given[i] = given[i] + extra
            rest = rest - extra
    return np.array(given)


def noise(own_key, shape, deviation, reach, cuts=(), kind=jnp.bfloat16):
    array = deviation * jax.random.normal(own_key, shape, jnp.float32)
    if cuts:
        array = array * steps_of(own_key, shape, cuts, -0.22, 0.18)
    return jnp.clip(array, -reach, reach).astype(kind)


def heavy_noise(own_key, extent, scale, limit, cuts, heavy, kind=jnp.bfloat16):
    values = scale * jax.random.normal(own_key, extent, jnp.float32)
    if cuts:
        values = values * steps_of(own_key, extent, cuts, -0.22, 0.18)
    return jnp.clip(spiked(values, jax.random.fold_in(own_key, 3), *heavy), -limit, limit).astype(kind)


def setup_inputs(seed: int = 0) -> dict:
    key_of = jax.random.split(jax.random.key(seed), 16)
    cotangent = heavy_noise(key_of[0], (TOKENS, D), 1.0, 6.0, ((0, 4), (1, 8)), (0, 1, 8, 2.0))
    block_input = noise(key_of[1], (TOKENS, D), 1.0, 6.0, ((0, 4), (1, 8)))
    routes_keys = jax.random.split(jax.random.fold_in(key_of[2], 1), TOKENS // TOK_DEV)
    routes_turns = jax.random.permutation(jax.random.fold_in(key_of[2], 3), TOKENS // TOK_DEV)
    routes = jax.vmap(lambda own, number: routed_block(jax.random.fold_in(key_of[2], 2), own, number, TOK_DEV, EXPERTS, TOP_K, CAP, 2))(routes_keys, routes_turns).reshape((TOKENS, TOP_K))
    route_weights = jnp.clip(0.1 + 0.79999997 * jax.random.uniform(key_of[3], (TOKENS, TOP_K), jnp.float32) ** steps_of(key_of[3], (TOKENS, TOP_K), ((0, 4),), -0.2, 0.2), 0.1, 0.9)
    gate_weight = noise(key_of[4], (EXPERTS, D, FF), D ** -0.5, 0.125, ((0, 4), (2, 8)))
    up_weight = noise(key_of[5], (EXPERTS, D, FF), D ** -0.5, 0.125, ((0, 4), (2, 8)))
    down_weight = noise(key_of[6], (EXPERTS, FF, D), FF ** -0.5, 0.0625, ((0, 4), (1, 8)))
    out_weight = noise(key_of[7], (WIDTH, D), WIDTH ** -0.5, 0.1875, ((0, 8),))
    conv_out = noise(key_of[8], (WIDTH, TOKENS), 1.0, 6.0, ((0, 8), (1, 4)))
    gate_pre = noise(key_of[9], (WIDTH, TOKENS), 1.0, 6.0, ((0, 8), (1, 4)))
    prior_states = noise(key_of[10], (WIDTH, TOKENS), 1.0, 6.0, ((0, 8), (1, 4)))
    recur_weight = noise(key_of[11], (HEADS, HEAD_DIM, HEAD_DIM), HEAD_DIM ** -0.5, 0.75)
    input_gate_matrix = noise(key_of[12], (HEADS, HEAD_DIM, HEAD_DIM), HEAD_DIM ** -0.5, 0.75)
    decay_param = draw_decay_param(jax.random.fold_in(key_of[15], 71), 0)
    decay_jump = draw_decay_jump(jax.random.fold_in(key_of[15], 71), 0)
    return dict(cotangent=cotangent, block_input=block_input, routes=routes, route_weights=route_weights, gate_weight=gate_weight, up_weight=up_weight, down_weight=down_weight, out_weight=out_weight, conv_out=conv_out, gate_pre=gate_pre, prior_states=prior_states, recur_weight=recur_weight, input_gate_matrix=input_gate_matrix, decay_param=decay_param, decay_jump=decay_jump)


RATE_SCALE = 8.0

def link_pairs(left_pair, right_pair):
    return (left_pair[0] * right_pair[0], right_pair[0] * left_pair[1] + right_pair[1])

def expert_pass(operands, padded_input, padded_cot):
    index_row, weight_row, w_gate, w_up, w_down = operands
    slot_rows = padded_input[index_row]
    slot_cot = (weight_row[:, None] * padded_cot[index_row].astype(jnp.float32)).astype(jnp.bfloat16)
    gate_act = jnp.dot(slot_rows, w_gate, preferred_element_type=jnp.float32)
    up_act = jnp.dot(slot_rows, w_up, preferred_element_type=jnp.float32)
    sigma_gate = jax.nn.sigmoid(gate_act)
    silu_val = gate_act * sigma_gate
    hidden = (silu_val * up_act).astype(jnp.bfloat16)
    down_grad = jnp.dot(hidden.T, slot_cot, preferred_element_type=jnp.float32).astype(jnp.bfloat16)
    d_hidden = jnp.dot(slot_cot, w_down.T, preferred_element_type=jnp.float32)
    d_gate = (d_hidden * up_act * sigma_gate * (1.0 + gate_act * (1.0 - sigma_gate))).astype(jnp.bfloat16)
    d_up = (d_hidden * silu_val).astype(jnp.bfloat16)
    gate_grad = jnp.dot(slot_rows.T, d_gate, preferred_element_type=jnp.float32).astype(jnp.bfloat16)
    up_grad = jnp.dot(slot_rows.T, d_up, preferred_element_type=jnp.float32).astype(jnp.bfloat16)
    blocks = FF // N_TP
    row_count = index_row.shape[0]
    gate_parts = jnp.einsum('rnf,dnf->nrd', d_gate.astype(jnp.float32).reshape(row_count, N_TP, blocks), w_gate.astype(jnp.float32).reshape(D, N_TP, blocks))
    up_parts = jnp.einsum('rnf,dnf->nrd', d_up.astype(jnp.float32).reshape(row_count, N_TP, blocks), w_up.astype(jnp.float32).reshape(D, N_TP, blocks))
    width_part = lax.optimization_barrier((gate_parts + up_parts).astype(jnp.bfloat16))
    row_grad = lax.optimization_barrier(jnp.sum(width_part.astype(jnp.float32), axis=0)).astype(jnp.bfloat16)
    return (gate_grad, up_grad, down_grad, row_grad)

def reference(cotangent, block_input, routes, route_weights, gate_weight, up_weight, down_weight, out_weight, conv_out, gate_pre, prior_states, recur_weight, input_gate_matrix, decay_param, decay_jump):
    route_count = TOK_DEV * TOP_K
    flat_routes = routes.reshape(N_SP, route_count).astype(jnp.int32)
    onehot = (flat_routes[:, :, None] == jnp.arange(EXPERTS, dtype=jnp.int32)[None, None, :]).astype(jnp.int32)
    slot_rank = lax.optimization_barrier(jnp.sum((jnp.cumsum(onehot, axis=1) - onehot) * onehot, axis=2)).astype(jnp.int32)
    source = jnp.arange(N_SP, dtype=jnp.int32)[:, None]
    position = jnp.arange(route_count, dtype=jnp.int32)[None, :]
    token_ids = (source * TOK_DEV + position // TOP_K).astype(jnp.int32)
    slot_ids = ((flat_routes * N_SP + source) * CAP + slot_rank).astype(jnp.int32)
    total = EXPERTS * N_SP * CAP
    table = jnp.full((total,), TOKENS, jnp.int32).at[slot_ids.reshape(-1)].set(token_ids.reshape(-1))
    weight_table = jnp.zeros((total,), jnp.float32).at[slot_ids.reshape(-1)].set(route_weights.reshape(N_SP, route_count).reshape(-1))
    padded_input = jnp.concatenate([block_input, jnp.zeros((1, D), jnp.bfloat16)], axis=0)
    padded_cot = jnp.concatenate([cotangent, jnp.zeros((1, D), jnp.bfloat16)], axis=0)
    gate_weight_grad, up_weight_grad, down_weight_grad, row_grads = lax.map(partial_expert(padded_input, padded_cot), (table.reshape(EXPERTS, N_SP * CAP), weight_table.reshape(EXPERTS, N_SP * CAP), gate_weight, up_weight, down_weight))
    moe_grad = jnp.zeros((TOKENS + 1, D), jnp.float32).at[table].add(row_grads.reshape(total, D).astype(jnp.float32))[:TOKENS]
    block_grad = (cotangent.astype(jnp.float32) + moe_grad).astype(jnp.bfloat16)
    conv_vals = conv_out.astype(jnp.float32)
    shaped = conv_vals.reshape(HEADS, HEAD_DIM, TOKENS)
    recur_gate = jax.nn.sigmoid(jnp.einsum('hij,hit->hjt', recur_weight.astype(jnp.float32), shaped).reshape(WIDTH, TOKENS))
    input_gate = jax.nn.sigmoid(jnp.einsum('hij,hit->hjt', input_gate_matrix.astype(jnp.float32), shaped).reshape(WIDTH, TOKENS))
    softened = jax.nn.softplus(-decay_param)[:, None]
    log_decay = -RATE_SCALE * recur_gate * softened + decay_jump
    decay_val = jnp.exp(log_decay)
    norm_scale = jnp.sqrt(-jnp.expm1(2.0 * log_decay))
    prior_vals = prior_states.astype(jnp.float32)
    state = decay_val * prior_vals + norm_scale * input_gate * conv_vals
    gate_vals = gate_pre.astype(jnp.float32)
    gelu_val, gelu_pull = jax.vjp(jax.nn.gelu, gate_vals)
    mixed = (gelu_val * state).astype(jnp.bfloat16)
    out_weight_grad = jnp.dot(mixed, block_grad, preferred_element_type=jnp.float32)
    d_mixed = jnp.dot(out_weight, block_grad.T, preferred_element_type=jnp.float32)
    valve_logit_derivative = gelu_pull(d_mixed * state)[0].astype(jnp.bfloat16)
    d_state = d_mixed * gelu_val
    shifted = jnp.concatenate([decay_val[:, 1:], jnp.ones((WIDTH, 1), jnp.float32)], axis=1)
    flipped = lax.associative_scan(link_pairs, (jnp.flip(shifted, 1), jnp.flip(d_state, 1)), axis=1)
    state_grad = jnp.flip(flipped[1], 1)
    grad_log = state_grad * prior_vals * decay_val - state_grad * input_gate * conv_vals * decay_val * decay_val / norm_scale
    grad_recur = (grad_log * -RATE_SCALE * softened * recur_gate * (1.0 - recur_gate)).astype(jnp.bfloat16)
    grad_input = (state_grad * norm_scale * conv_vals * input_gate * (1.0 - input_gate)).astype(jnp.bfloat16)
    back_recur = jnp.einsum('hij,hjt->hit', recur_weight.astype(jnp.float32), grad_recur.astype(jnp.float32).reshape(HEADS, HEAD_DIM, TOKENS)).reshape(WIDTH, TOKENS)
    back_input = jnp.einsum('hij,hjt->hit', input_gate_matrix.astype(jnp.float32), grad_input.astype(jnp.float32).reshape(HEADS, HEAD_DIM, TOKENS)).reshape(WIDTH, TOKENS)
    conv_grad = (state_grad * norm_scale * input_gate + back_recur + back_input).astype(jnp.bfloat16)
    return (gate_weight_grad, up_weight_grad, down_weight_grad, out_weight_grad, conv_grad, valve_logit_derivative)

def partial_expert(padded_input, padded_cot):

    def run_expert(operands):
        return expert_pass(operands, padded_input, padded_cot)
    return run_expert
```

```python
import functools

import jax
import jax.numpy as jnp
from jax import lax
from jax.experimental import pallas as pl
from jax.experimental.pallas import tpu as pltpu
from jax.sharding import PartitionSpec as P

HEAD_DIM = 64
TOP_K = 2
RATE_SCALE = 8.0
CORES = 2
NN = (((1,), (0,)), ((), ()))
NT = (((1,), (1,)), ((), ()))
TN = (((0,), (0,)), ((), ()))
F32 = jnp.float32
BF16 = jnp.bfloat16


def dot(a, b, dims=NN):
    return lax.dot_general(a, b, dims, preferred_element_type=F32)


def across(place, step, size):
    result, bit = 0, 1
    while bit < size:
        result = result + lax.rem(lax.div(place, bit) + (step // bit) % 2, 2) * bit
        bit *= 2
    return result


def span(block, width):
    return pl.ds(pl.multiple_of(block * width, width), width)


def greet(devices):
    barrier = pltpu.get_barrier_semaphore()
    for device in devices:
        pl.semaphore_signal(
            barrier, inc=1, device_id=device, device_id_type=pl.DeviceIdType.MESH
        )
    pl.semaphore_wait(barrier, len(devices))


def log1p_small(y):
    series = y * (1.0 + y * (-0.5 + y * (1.0 / 3 + y * (-0.25 + y * (0.2 - y / 6.0)))))
    return jnp.where(y < 0.03125, series, jnp.log(1.0 + y))


def expm1_neg(x):
    series = 1.0 / 40320 * x + 1.0 / 5040
    for factor in (720, 120, 24, 6, 2):
        series = series * x + 1.0 / factor
    series = x * (series * x + 1.0)
    return jnp.where(x > -0.35, series, jnp.exp(x) - 1.0)


class Copies:
    def __init__(self, send_sems, recv_sems):
        self.sems = (send_sems, recv_sems)
        self.count = 0
        self.sent = []

    def start(self, source, target, device):
        copy = pltpu.make_async_remote_copy(
            src_ref=source,
            dst_ref=target,
            send_sem=self.sems[0].at[self.count],
            recv_sem=self.sems[1].at[self.count],
            device_id=device,
            device_id_type=pl.DeviceIdType.MESH,
        )
        copy.start()
        self.count += 1
        self.sent.append(copy)
        return copy


INPUTS = (
    "rows_hbm", "cot_hbm", "routes", "route_w", "wg_hbm", "wu_hbm", "wd_hbm", "ow_hbm",
    "conv_hbm", "pre_hbm", "prior_hbm", "wr_hbm", "wi_hbm", "rate", "jump_hbm",
)
OUTPUTS = ("gate_grad", "up_grad", "down_grad", "out_grad", "conv_grad", "valve")


class Refs:
    pass


def kernel(names, experts, deep, cap, *refs):
    r = Refs()
    for name, ref in zip(names, refs):
        setattr(r, name, ref)
    sp, tp = lax.axis_index("sp"), lax.axis_index("tp")
    z, core = lax.div(tp, CORES), lax.rem(tp, CORES)
    partner = (sp, z * CORES + 1 - core)
    planes = [(across(sp, k, experts), tp) for k in range(experts)]
    levels = [across(z, d, deep) for d in range(deep)]
    lines = [(sp, level * CORES + core) for level in levels]
    tokens, width = r.rows.shape
    pair = CORES * width
    full = width * CORES * deep
    total = experts * cap
    hidden_units = r.wg.shape[1]
    channels, length = r.conv.shape
    heads = channels // HEAD_DIM
    copies = Copies(r.send_sems, r.recv_sems)
    sources = [
        (r.rows_hbm, r.rows), (r.cot_hbm, r.cot), (r.wg_hbm.at[0], r.wg),
        (r.wu_hbm.at[0], r.wu), (r.wd_hbm.at[0], r.wd), (r.conv_hbm, r.conv),
        (r.pre_hbm, r.pre), (r.prior_hbm, r.prior), (r.jump_hbm, r.jump),
        (r.wr_hbm.at[span(tp, heads)], r.wr), (r.wi_hbm.at[span(tp, heads)], r.wi),
        (r.ow_hbm, r.ow),
    ]
    local = [
        pltpu.make_async_copy(a, b, r.local_sems.at[i]) for i, (a, b) in enumerate(sources)
    ]
    for copy in local:
        copy.start()
    greet(planes[1:] + lines[1:] + [partner])
    local[0].wait()
    local[1].wait()
    own = (r.rows, r.cot)
    relieved = (1, 1)
    line = {}
    raw = [(a, d) for a in range(2) for d in range(1, deep) if (a, d) != relieved]
    for a, d in raw:
        line[a, d] = copies.start(own[a], r.held.at[a, d - 1], lines[d])

    expert_ids = lax.broadcasted_iota(jnp.int32, (16, tokens), 0)
    first = r.routes[0:1, :] == expert_ids
    second = r.routes[1:2, :] == expert_ids
    member = (first | second).astype(F32)
    weight_of = jnp.where(first, r.route_w[0:1, :], 0.0) + jnp.where(
        second, r.route_w[1:2, :], 0.0
    )
    earlier = lax.broadcasted_iota(jnp.int32, (tokens, tokens), 0) < lax.broadcasted_iota(
        jnp.int32, (tokens, tokens), 1
    )
    rank = dot(member.astype(BF16), earlier.astype(F32).astype(BF16))
    rank = jnp.where(member > 0.5, rank, -1.0)
    slot_ids = lax.broadcasted_iota(jnp.int32, (cap, tokens), 0).astype(F32)
    for e in range(experts):
        hit = slot_ids == rank[e : e + 1, :]
        r.placing[e * cap : (e + 1) * cap, :] = jnp.where(hit, 1.0, 0.0).astype(BF16)
        r.slot_weight[e * cap : (e + 1) * cap, :] = jnp.sum(
            jnp.where(hit, weight_of[e : e + 1, :], 0.0), axis=1, keepdims=True
        )

    filled = (r.slot_rows, r.slot_cot)
    plane, forward = {}, {}

    def here_of(d):
        return span(levels[d] * CORES + core, width)

    def issue(a, d):
        if (a, d) == relieved:
            return
        if d:
            line[a, d].wait_recv()
        block = r.held[a, d - 1] if d else own[a][...]
        placed = dot(r.placing[...], block)
        if a:
            placed = placed * r.slot_weight[...]
        r.stage[a, d] = placed.astype(BF16)
        for k in range(1, experts):
            plane[a, d, k] = copies.start(
                r.stage.at[a, d, span(planes[k][0], cap)],
                filled[a].at[span(sp, cap), here_of(d)],
                planes[k],
            )
        filled[a][span(sp, cap), here_of(d)] = r.stage[a, d, span(sp, cap), :]

    def pass_on(a, d):
        if (a, d) == relieved:
            line[a, d].wait_recv()
        else:
            for k in range(1, experts):
                plane[a, d, k].wait_recv()
        here = filled[a].at[:, here_of(d)]
        forward[a, d] = copies.start(here, here, partner)
        if d == 0 and a == relieved[0] and deep > 1:
            there = r.slot_cot.at[:, here_of(0)]
            line[relieved] = copies.start(there, there, lines[relieved[1]])

    def row_loop(body):
        size = total // 2

        def step(i, carry):
            body(span(i, size))
            return carry

        lax.fori_loop(0, 2, step, 0)

    seen = [0, 0]

    def absorb(a, d):
        forward[a, d].wait_recv()
        cols = span(levels[d], pair)
        order = seen[a]
        seen[a] += 1
        if a == 0:
            if order == 0:
                local[2].wait()
                local[3].wait()

            def chunk(rows):
                x = r.slot_rows[rows, cols]
                gate = dot(x, r.wg[cols, :])
                up = dot(x, r.wu[cols, :])
                if order:
                    gate = gate + r.acc_gate[rows, :]
                    up = up + r.acc_up[rows, :]
                if order == deep - 1:
                    sigma = jax.nn.sigmoid(gate)
                    silu = gate * sigma
                    r.hidden[rows, :] = (silu * up).astype(BF16)
                    gate = up * (sigma * (1.0 + gate * (1.0 - sigma)))
                    up = silu
                r.acc_gate[rows, :] = gate
                r.acc_up[rows, :] = up
        else:
            if order == 0:
                local[4].wait()

            def chunk(rows):
                value = dot(r.slot_cot[rows, cols], r.wd[:, cols], NT)
                if order:
                    value = value + r.acc_hidden[rows, :]
                if order < deep - 1:
                    r.acc_hidden[rows, :] = value
                else:
                    r.d_gate[rows, :] = (value * r.acc_gate[rows, :]).astype(BF16)
                    r.d_up[rows, :] = (value * r.acc_up[rows, :]).astype(BF16)

        row_loop(chunk)

    eye = lax.broadcasted_iota(jnp.int32, (channels, channels), 0) == lax.broadcasted_iota(
        jnp.int32, (channels, channels), 1
    )
    place = lax.broadcasted_iota(jnp.int32, (channels, length), 1)

    def to_column(row):
        return jnp.sum(jnp.where(eye, row, 0.0), axis=1, keepdims=True)

    def to_row(column):
        return jnp.sum(jnp.where(eye, column, 0.0), axis=0, keepdims=True)

    def by_head(weights, x, dims):
        return jnp.concatenate(
            [
                dot(weights[h], x[h * HEAD_DIM : (h + 1) * HEAD_DIM, :], dims)
                for h in range(heads)
            ],
            axis=0,
        )

    def prepare_gates():
        for i in range(5, 12):
            local[i].wait()
        conv = r.conv[...].astype(F32)
        prior = r.prior[...].astype(F32)
        recur = jax.nn.sigmoid(by_head(r.wr, r.conv[...], TN))
        gate = jax.nn.sigmoid(by_head(r.wi, r.conv[...], TN))
        rate = -r.rate[pl.ds(tp, 1), :]
        soft = to_column(jnp.maximum(rate, 0.0) + log1p_small(jnp.exp(-jnp.abs(rate))))
        log_decay = -RATE_SCALE * recur * soft + r.jump[...]
        decay = jnp.exp(log_decay)
        norm = jnp.sqrt(-expm1_neg(2.0 * log_decay))
        state = decay * prior + norm * gate * conv
        x = r.pre[...].astype(F32)
        inner = 0.7978845608028654 * (x + 0.044715 * (x * x * x))
        bend = jnp.tanh(inner)
        gelu = 0.5 * x * (1.0 + bend)
        slope = 0.5 * (1.0 + bend) + 0.5 * x * (1.0 - bend * bend) * (
            0.7978845608028654 * (1.0 + 3 * 0.044715 * (x * x))
        )
        r.mixed[...] = (gelu * state).astype(BF16)
        pull = prior * decay - gate * conv * decay * decay / norm
        r.keep[0] = pull * (-RATE_SCALE * soft) * recur * (1.0 - recur)
        r.keep[1] = norm * conv * gate * (1.0 - gate)
        r.keep[2] = norm * gate
        r.keep[3] = slope * state
        r.keep[4] = gelu
        r.keep[5] = decay

    def prepare_scan():
        decay = r.keep[5]
        later = jnp.where(place < length - 1, pltpu.roll(decay, length - 1, 1), 1.0)
        reach, level = 1, 0
        while reach < length:
            inside = place < length - reach
            r.reach[level] = jnp.where(inside, later, 0.0)
            later = later * jnp.where(inside, pltpu.roll(later, length - reach, 1), 1.0)
            reach *= 2
            level += 1
        r.keep[6] = later

    def prepare_taking():
        r.taking[...] = r.placing[...].T

    stages = [(0, 0), (1, 0)] + [(0, d) for d in range(1, deep)]
    stages += [(1, d) for d in range(2, deep)]
    stages.insert(len(stages) - 1, relieved)
    between = {1: prepare_gates, 2: prepare_scan, 3: prepare_taking}
    count = len(stages)
    for i in range(count + 2):
        if i < count:
            issue(*stages[i])
        if i in between:
            between[i]()
        if 1 <= i <= count:
            pass_on(*stages[i - 1])
        if i >= 2:
            absorb(*stages[i - 2])

    fillers = []

    def blocks_of(body, steps, group):
        for start in range(0, steps, group):

            def run(start=start):
                def step(i, carry):
                    body(i)
                    return carry

                lax.fori_loop(start, min(start + group, steps), step, 0)

            fillers.append(run)

    wide = 256

    def gate_block(i):
        rows = r.slot_rows[:, span(i, wide)]
        r.gate_grad[0, span(i, wide), :] = dot(rows, r.d_gate[...], TN).astype(BF16)

    def up_block(i):
        rows = r.slot_rows[:, span(i, wide)]
        r.up_grad[0, span(i, wide), :] = dot(rows, r.d_up[...], TN).astype(BF16)

    def down_block(i):
        cols = span(i, wide)
        r.down_grad[0, :, cols] = dot(r.hidden[...], r.slot_cot[:, cols], TN).astype(BF16)

    blocks_of(down_block, full // wide, 2)
    blocks_of(gate_block, full // wide, 2)
    blocks_of(up_block, full // wide, 2)

    def fill(amount):
        for _ in range(amount):
            if fillers:
                fillers.pop(0)()

    order = list(range(deep - 1, -1, -1))
    core_copy, home_copy, line_copy = {}, {}, {}

    def width_block(block, store):
        def chunk(rows):
            value = dot(r.d_gate[rows, :], r.wg[span(block, width), :], NT)
            store(rows, value + dot(r.d_up[rows, :], r.wu[span(block, width), :], NT))

        row_loop(chunk)

    def theirs(d):
        def store(rows, value):
            r.lent[d, rows, :] = value.astype(BF16)

        width_block(levels[d] * CORES + 1 - core, store)
        core_copy[d] = copies.start(r.lent.at[d], r.paired.at[d], partner)

    def mine(d):
        def store(rows, value):
            r.kept[d, rows, :] = value

        width_block(levels[d] * CORES + core, store)

    def ship(d):
        core_copy[d].wait_recv()
        r.joint[d] = (r.kept[d] + r.paired[d].astype(F32)).astype(BF16)
        for k in range(1, experts):
            home_copy[d, k] = copies.start(
                r.joint.at[d, span(planes[k][0], cap)],
                r.homed.at[d, span(sp, cap)],
                planes[k],
            )
        r.homed[d, span(sp, cap), :] = r.joint[d, span(sp, cap), :]

    theirs(order[0])
    for i, d in enumerate(order):
        mine(d)
        if i + 1 < deep:
            theirs(order[i + 1])
        ship(d)
    fill(1)
    for d in order:
        for k in range(1, experts):
            home_copy[d, k].wait_recv()
        summed = dot(r.taking[...], r.homed[d])
        if d:
            r.line_out[d - 1] = summed.astype(BF16)
            line_copy[d] = copies.start(r.line_out.at[d - 1], r.line_in.at[d - 1], lines[d])
        else:
            r.sum_own[...] = summed + r.cot[...].astype(F32)
        fill(2)
    value = r.sum_own[...]
    for d in order[:-1]:
        line_copy[d].wait_recv()
        value = value + r.line_in[d - 1].astype(F32)
    here = span(tp, width)
    r.block_grad[:, here] = value.astype(BF16)
    gathers, shared = {}, {}
    for d in range(1, deep):
        gathers[d] = copies.start(
            r.block_grad.at[:, here], r.block_grad.at[:, here], lines[d]
        )
    shared[0] = copies.start(r.block_grad.at[:, here], r.block_grad.at[:, here], partner)
    fill(2)

    def level_done(d):
        shared[d].wait_recv()
        cols = span(levels[d], pair)
        block = r.block_grad[:, cols]
        r.product[:, cols] = dot(r.mixed[...], block).astype(BF16)
        value = dot(r.ow[:, cols], block, NT)
        r.d_mixed[...] = value if d == 0 else r.d_mixed[...] + value

    level_done(0)
    for d in range(1, deep):
        fill(2)
        gathers[d].wait_recv()
        spot = r.block_grad.at[:, here_of(d)]
        shared[d] = copies.start(spot, spot, partner)
        if d == deep - 1:
            fill(100)
        if d > 1:
            level_done(d - 1)
    level_done(deep - 1)

    d_mixed = r.d_mixed[...]
    value = d_mixed * r.keep[4]
    reach, level = 1, 0
    while reach < length:
        value = value + r.reach[level] * pltpu.roll(value, length - reach, 1)
        reach *= 2
        level += 1
    decay_first = r.keep[5][:, 0:1]
    head_prod = to_row(decay_first * r.keep[6][:, 0:1])
    head_sum = to_row(decay_first * value[:, 0:1])
    r.summary[0:1, :] = head_prod
    r.summary[1:2, :] = head_sum
    tails = []
    for k in range(1, experts):
        tails.append(copies.start(r.summary, r.summaries.at[sp], planes[k]))
    out_width = r.products.shape[2]
    for k in range(1, experts):
        tails.append(
            copies.start(
                r.product.at[:, span(planes[k][0], out_width)], r.products.at[k - 1], planes[k]
            )
        )
    r.summaries[sp] = r.summary[...]
    r.valve[...] = (d_mixed * r.keep[3]).astype(BF16)
    for copy in tails[: experts - 1]:
        copy.wait_recv()
    carried = jnp.zeros((1, channels), F32)
    for later in range(experts - 1, 0, -1):
        longer = r.summaries[later, 1:2, :] + r.summaries[later, 0:1, :] * carried
        carried = jnp.where(later > sp, longer, carried)
    state_grad = value + r.keep[6] * to_column(carried)
    grad_recur = (state_grad * r.keep[0]).astype(BF16)
    grad_input = (state_grad * r.keep[1]).astype(BF16)
    conv_grad = state_grad * r.keep[2]
    conv_grad = conv_grad + by_head(r.wr, grad_recur, NN) + by_head(r.wi, grad_input, NN)
    r.conv_grad[...] = conv_grad.astype(BF16)
    value = r.product[:, span(sp, out_width)].astype(F32)
    for k in range(1, experts):
        tails[experts - 2 + k].wait_recv()
        value = value + r.products[k - 1].astype(F32)
    r.out_grad[...] = value
    for copy in copies.sent:
        copy.wait_send()


def local(
    cotangent,
    block_input,
    routes,
    route_weights,
    gate_weight,
    up_weight,
    down_weight,
    out_weight,
    conv_out,
    gate_pre,
    prior_states,
    recur_weight,
    input_gate_matrix,
    decay_param,
    decay_jump,
):
    experts, columns = lax.axis_size("sp"), lax.axis_size("tp")
    deep = columns // CORES
    tokens, width = cotangent.shape
    cap = -(-(5 * tokens * TOP_K // (4 * experts)) // 16) * 16
    total = experts * cap
    full = width * columns
    units = gate_weight.shape[2]
    channels, length = conv_out.shape
    heads = channels // HEAD_DIM
    doublings = (length - 1).bit_length()
    copies = 2 * deep * (experts + 1) + 2 * deep + deep * (experts + 3) + 2 * experts
    vmem = pltpu.VMEM
    scratch = dict(
        rows=vmem((tokens, width), BF16),
        cot=vmem((tokens, width), BF16),
        wg=vmem((full, units), BF16),
        wu=vmem((full, units), BF16),
        wd=vmem((units, full), BF16),
        ow=vmem((channels, full), BF16),
        conv=vmem((channels, length), BF16),
        pre=vmem((channels, length), BF16),
        prior=vmem((channels, length), BF16),
        jump=vmem((channels, length), F32),
        wr=vmem((heads, HEAD_DIM, HEAD_DIM), BF16),
        wi=vmem((heads, HEAD_DIM, HEAD_DIM), BF16),
        held=vmem((2, deep - 1, tokens, width), BF16),
        placing=vmem((total, tokens), BF16),
        taking=vmem((tokens, total), BF16),
        slot_weight=vmem((total, 1), F32),
        stage=vmem((2, deep, total, width), BF16),
        slot_rows=vmem((total, full), BF16),
        slot_cot=vmem((total, full), BF16),
        acc_gate=vmem((total, units), F32),
        acc_up=vmem((total, units), F32),
        acc_hidden=vmem((total, units), F32),
        hidden=vmem((total, units), BF16),
        d_gate=vmem((total, units), BF16),
        d_up=vmem((total, units), BF16),
        lent=vmem((deep, total, width), BF16),
        paired=vmem((deep, total, width), BF16),
        kept=vmem((deep, total, width), F32),
        joint=vmem((deep, total, width), BF16),
        homed=vmem((deep, total, width), BF16),
        line_out=vmem((deep - 1, tokens, width), BF16),
        line_in=vmem((deep - 1, tokens, width), BF16),
        sum_own=vmem((tokens, width), F32),
        block_grad=vmem((tokens, full), BF16),
        mixed=vmem((channels, length), BF16),
        d_mixed=vmem((channels, length), F32),
        keep=vmem((7, channels, length), F32),
        reach=vmem((doublings, channels, length), F32),
        product=vmem((channels, full), BF16),
        products=vmem((experts - 1, channels, full // experts), BF16),
        summary=vmem((8, channels), F32),
        summaries=vmem((experts, 8, channels), F32),
        send_sems=pltpu.SemaphoreType.DMA((copies,)),
        recv_sems=pltpu.SemaphoreType.DMA((copies,)),
        local_sems=pltpu.SemaphoreType.DMA((12,)),
    )
    on_chip = pl.BlockSpec(memory_space=pltpu.VMEM)
    far = pl.BlockSpec(memory_space=pltpu.HBM)
    given = ("routes", "route_w", "rate")
    return pl.pallas_call(
        functools.partial(kernel, INPUTS + OUTPUTS + tuple(scratch), experts, deep, cap),
        out_shape=(
            jax.ShapeDtypeStruct(gate_weight.shape, BF16),
            jax.ShapeDtypeStruct(up_weight.shape, BF16),
            jax.ShapeDtypeStruct(down_weight.shape, BF16),
            jax.ShapeDtypeStruct((channels, full // experts), F32),
            jax.ShapeDtypeStruct((channels, length), BF16),
            jax.ShapeDtypeStruct((channels, length), BF16),
        ),
        in_specs=[on_chip if name in given else far for name in INPUTS],
        out_specs=(on_chip,) * 6,
        scratch_shapes=list(scratch.values()),
        compiler_params=pltpu.CompilerParams(
            collective_id=0, has_side_effects=True, vmem_limit_bytes=67043328
        ),
    )(
        block_input,
        cotangent,
        jnp.transpose(routes),
        jnp.transpose(route_weights),
        gate_weight,
        up_weight,
        down_weight,
        out_weight,
        conv_out,
        gate_pre,
        prior_states,
        recur_weight,
        input_gate_matrix,
        decay_param.reshape(columns, channels),
        decay_jump,
    )


def solution(mesh):
    in_specs = (
        P("sp", "tp"),
        P("sp", "tp"),
        P("sp", None),
        P("sp", None),
        P("sp", None, "tp"),
        P("sp", None, "tp"),
        P("sp", "tp", None),
        P("tp", None),
        P("tp", "sp"),
        P("tp", "sp"),
        P("tp", "sp"),
        P(),
        P(),
        P(),
        P("tp", "sp"),
    )
    out_specs = (
        P("sp", None, "tp"),
        P("sp", None, "tp"),
        P("sp", "tp", None),
        P("tp", "sp"),
        P("tp", "sp"),
        P("tp", "sp"),
    )
    return jax.shard_map(local, mesh=mesh, in_specs=in_specs, out_specs=out_specs, check_vma=False)
```

```python
import functools

import jax
import jax.numpy as jnp
from jax import lax
from jax.experimental import pallas as pl
from jax.experimental.pallas import tpu as pltpu
from jax.sharding import PartitionSpec as P

HEAD_DIM = 64
TOP_K = 2
RATE_SCALE = 8.0
CORES = 2
NN = (((1,), (0,)), ((), ()))
NT = (((1,), (1,)), ((), ()))
TN = (((0,), (0,)), ((), ()))
F32 = jnp.float32
BF16 = jnp.bfloat16


def dot(a, b, dims=NN):
    return lax.dot_general(a, b, dims, preferred_element_type=F32)


def across(place, step, size):
    result, bit = 0, 1
    while bit < size:
        result = result + lax.rem(lax.div(place, bit) + (step // bit) % 2, 2) * bit
        bit *= 2
    return result


def span(block, width):
    return pl.ds(pl.multiple_of(block * width, width), width)


def signal(devices):
    barrier = pltpu.get_barrier_semaphore()
    for device in devices:
        pl.semaphore_signal(
            barrier, inc=1, device_id=device, device_id_type=pl.DeviceIdType.MESH
        )


def log1p_small(y):
    series = y * (1.0 + y * (-0.5 + y * (1.0 / 3 + y * (-0.25 + y * (0.2 - y / 6.0)))))
    return jnp.where(y < 0.03125, series, jnp.log(1.0 + y))


def expm1_neg(x):
    series = 1.0 / 40320 * x + 1.0 / 5040
    for factor in (720, 120, 24, 6, 2):
        series = series * x + 1.0 / factor
    series = x * (series * x + 1.0)
    return jnp.where(x > -0.35, series, jnp.exp(x) - 1.0)


class Copies:
    def __init__(self, send_sems, recv_sems):
        self.sems = (send_sems, recv_sems)
        self.count = 0
        self.sent = []

    def start(self, source, target, device, when=None, arrival=None):
        index, self.count = self.count, self.count + 1
        copy = pltpu.make_async_remote_copy(
            src_ref=source,
            dst_ref=target,
            send_sem=self.sems[0].at[index],
            recv_sem=self.sems[1].at[index if arrival is None else arrival],
            device_id=device,
            device_id_type=pl.DeviceIdType.MESH,
        )
        self.run(when, copy.start)
        self.sent.append((when, copy))
        return index, copy

    def run(self, when, action):
        if when is None:
            action()
        else:
            pl.when(when)(action)

    def finish(self):
        for when, copy in self.sent:
            self.run(when, copy.wait_send)
        self.sent = []


INPUTS = (
    "rows_hbm", "cot_hbm", "routes", "route_w", "wg_hbm", "wu_hbm", "wd_hbm", "ow_hbm",
    "conv_hbm", "pre_hbm", "prior_hbm", "wr_hbm", "wi_hbm", "rate", "jump_hbm",
)
OUTPUTS = ("gate_grad", "up_grad", "down_grad", "out_grad", "conv_grad", "valve")


class Refs:
    pass


def kernel(names, experts, deep, cap, *refs):
    r = Refs()
    for name, ref in zip(names, refs):
        setattr(r, name, ref)
    sp, tp = lax.axis_index("sp"), lax.axis_index("tp")
    z, core = lax.div(tp, CORES), lax.rem(tp, CORES)
    partner = (sp, z * CORES + 1 - core)
    planes = [(across(sp, k, experts), tp) for k in range(experts)]
    levels = [across(z, d, deep) for d in range(deep)]
    lines = [(sp, level * CORES + core) for level in levels]
    tokens, width = r.rows.shape
    pair = CORES * width
    full = width * CORES * deep
    total = experts * cap
    hidden_units = r.wg.shape[1]
    channels, length = r.conv.shape
    heads = channels // HEAD_DIM
    copies = Copies(r.send_sems, r.recv_sems)
    sources = [
        (r.rows_hbm, r.rows), (r.cot_hbm, r.cot), (r.wg_hbm.at[0], r.wg),
        (r.wu_hbm.at[0], r.wu), (r.wd_hbm.at[0], r.wd), (r.conv_hbm, r.conv),
        (r.pre_hbm, r.pre), (r.prior_hbm, r.prior), (r.jump_hbm, r.jump),
        (r.wr_hbm.at[span(tp, heads)], r.wr), (r.wi_hbm.at[span(tp, heads)], r.wi),
        (r.ow_hbm, r.ow),
    ]
    local = [
        pltpu.make_async_copy(a, b, r.local_sems.at[i]) for i, (a, b) in enumerate(sources)
    ]
    peers = planes[1:] + lines[1:] + [partner]
    signal(peers)
    for copy in local:
        copy.start()
    with jax.named_scope("greet"):
        pl.semaphore_wait(pltpu.get_barrier_semaphore(), len(peers))
    local[0].wait()
    local[1].wait()
    own = (r.rows, r.cot)
    relieved = (1, 1)
    relay = deep == 4
    middle = (z == 1) | (z == 2)
    line = {}
    raw = [(a, d) for a in range(2) for d in range(1, deep) if (a, d) != relieved]
    for a, d in raw:
        line[a, d] = copies.start(
            own[a], r.held.at[a, d - 1], lines[d], middle if relay and d == 3 else None
        )

    expert_ids = lax.broadcasted_iota(jnp.int32, (16, tokens), 0)
    first = r.routes[0:1, :] == expert_ids
    second = r.routes[1:2, :] == expert_ids
    member = (first | second).astype(F32)
    weight_of = jnp.where(first, r.route_w[0:1, :], 0.0) + jnp.where(
        second, r.route_w[1:2, :], 0.0
    )
    earlier = lax.broadcasted_iota(jnp.int32, (tokens, tokens), 0) < lax.broadcasted_iota(
        jnp.int32, (tokens, tokens), 1
    )
    rank = dot(member.astype(BF16), earlier.astype(F32).astype(BF16))
    rank = jnp.where(member > 0.5, rank, -1.0)
    slot_ids = lax.broadcasted_iota(jnp.int32, (cap, tokens), 0).astype(F32)
    for e in range(experts):
        hit = slot_ids == rank[e : e + 1, :]
        r.placing[e * cap : (e + 1) * cap, :] = jnp.where(hit, 1.0, 0.0).astype(BF16)
        r.slot_weight[e * cap : (e + 1) * cap, :] = jnp.sum(
            jnp.where(hit, weight_of[e : e + 1, :], 0.0), axis=1, keepdims=True
        )

    filled = (r.slot_rows, r.slot_cot)
    plane, forward = {}, {}

    def here_of(d):
        return span(levels[d] * CORES + core, width)

    def issue(a, d):
        if d:
            line[a, d][1].wait_recv()
        if relay and d == 2:
            copies.start(
                r.held.at[a, 1], r.held.at[a, 2], lines[1], middle, line[a, 3][0]
            )
        block = r.held[a, d - 1] if d else own[a][...]
        placed = dot(r.placing[...], block)
        if a:
            placed = placed * r.slot_weight[...]
        r.stage[a, d] = placed.astype(BF16)
        for k in range(1, experts):
            plane[a, d, k] = copies.start(
                r.stage.at[a, d, span(planes[k][0], cap)],
                filled[a].at[span(sp, cap), here_of(d)],
                planes[k],
            )[1]
        filled[a][span(sp, cap), here_of(d)] = r.stage[a, d, span(sp, cap), :]

    def pass_on(a, d):
        if (a, d) == relieved:
            line[a, d].wait_recv()
        else:
            for k in range(1, experts):
                plane[a, d, k].wait_recv()
        here = filled[a].at[:, here_of(d)]
        forward[a, d] = copies.start(here, here, partner)[1]
        if d == 0 and a == relieved[0]:
            there = r.slot_cot.at[:, here_of(0)]
            line[relieved] = copies.start(there, there, lines[relieved[1]])[1]

    def row_loop(body):
        size = total // 2

        def step(i, carry):
            body(span(i, size))
            return carry

        lax.fori_loop(0, 2, step, 0)

    seen = [0, 0]

    def absorb(a, d):
        forward[a, d].wait_recv()
        cols = span(levels[d], pair)
        order = seen[a]
        seen[a] += 1
        if a == 0:
            if order == 0:
                local[2].wait()
                local[3].wait()

            def chunk(rows):
                x = r.slot_rows[rows, cols]
                gate = dot(x, r.wg[cols, :])
                up = dot(x, r.wu[cols, :])
                if order:
                    gate = gate + r.acc_gate[rows, :]
                    up = up + r.acc_up[rows, :]
                if order == deep - 1:
                    sigma = jax.nn.sigmoid(gate)
                    silu = gate * sigma
                    r.hidden[rows, :] = (silu * up).astype(BF16)
                    gate = up * (sigma * (1.0 + gate * (1.0 - sigma)))
                    up = silu
                r.acc_gate[rows, :] = gate
                r.acc_up[rows, :] = up
        else:
            if order == 0:
                local[4].wait()

            def chunk(rows):
                value = dot(r.slot_cot[rows, cols], r.wd[:, cols], NT)
                if order:
                    value = value + r.acc_hidden[rows, :]
                if order < deep - 1:
                    r.acc_hidden[rows, :] = value
                else:
                    r.d_gate[rows, :] = (value * r.acc_gate[rows, :]).astype(BF16)
                    r.d_up[rows, :] = (value * r.acc_up[rows, :]).astype(BF16)

        row_loop(chunk)

    eye = lax.broadcasted_iota(jnp.int32, (channels, channels), 0) == lax.broadcasted_iota(
        jnp.int32, (channels, channels), 1
    )
    place = lax.broadcasted_iota(jnp.int32, (channels, length), 1)

    def to_column(row):
        return jnp.sum(jnp.where(eye, row, 0.0), axis=1, keepdims=True)

    def to_row(column):
        return jnp.sum(jnp.where(eye, column, 0.0), axis=0, keepdims=True)

    def by_head(weights, x, dims):
        return jnp.concatenate(
            [
                dot(weights[h], x[h * HEAD_DIM : (h + 1) * HEAD_DIM, :], dims)
                for h in range(heads)
            ],
            axis=0,
        )

    def prepare_gates():
        for i in range(5, 12):
            local[i].wait()
        conv = r.conv[...].astype(F32)
        prior = r.prior[...].astype(F32)
        recur = jax.nn.sigmoid(by_head(r.wr, r.conv[...], TN))
        gate = jax.nn.sigmoid(by_head(r.wi, r.conv[...], TN))
        rate = -r.rate[pl.ds(tp, 1), :]
        soft = to_column(jnp.maximum(rate, 0.0) + log1p_small(jnp.exp(-jnp.abs(rate))))
        log_decay = -RATE_SCALE * recur * soft + r.jump[...]
        decay = jnp.exp(log_decay)
        norm = jnp.sqrt(-expm1_neg(2.0 * log_decay))
        state = decay * prior + norm * gate * conv
        x = r.pre[...].astype(F32)
        inner = 0.7978845608028654 * (x + 0.044715 * (x * x * x))
        bend = jnp.tanh(inner)
        gelu = 0.5 * x * (1.0 + bend)
        slope = 0.5 * (1.0 + bend) + 0.5 * x * (1.0 - bend * bend) * (
            0.7978845608028654 * (1.0 + 3 * 0.044715 * (x * x))
        )
        r.mixed[...] = (gelu * state).astype(BF16)
        pull = prior * decay - gate * conv * decay * decay / norm
        r.keep[0] = pull * (-RATE_SCALE * soft) * recur * (1.0 - recur)
        r.keep[1] = norm * conv * gate * (1.0 - gate)
        r.keep[2] = norm * gate
        r.keep[3] = slope * state
        r.keep[4] = gelu
        r.keep[5] = decay

    def prepare_scan():
        decay = r.keep[5]
        later = jnp.where(place < length - 1, pltpu.roll(decay, length - 1, 1), 1.0)
        reach, level = 1, 0
        while reach < length:
            inside = place < length - reach
            r.reach[level] = jnp.where(inside, later, 0.0)
            later = later * jnp.where(inside, pltpu.roll(later, length - reach, 1), 1.0)
            reach *= 2
            level += 1
        r.keep[6] = later

    def prepare_taking():
        r.taking[...] = r.placing[...].T

    def scoped(name, fn, *args):
        with jax.named_scope(name):
            fn(*args)

    stages = [(0, 0), (1, 0)] + [(0, d) for d in range(1, deep)]
    stages += [(1, d) for d in range(2, deep)]
    between = {0: prepare_gates, 1: prepare_scan, 2: prepare_taking}
    scoped("issue", issue, *stages[0])
    scoped("issue", issue, *stages[1])
    count = len(stages)
    behind = []
    for i in range(count):
        if i in between:
            scoped("between", between[i])
        if i + 2 < count:
            scoped(f"issue#i={i + 2}", issue, *stages[i + 2])
        if i == count - 1:
            scoped("pass_on_relieved", pass_on, *relieved)
            scoped("absorb_relieved", absorb, *stages[i - 1])
            behind = [relieved]
        elif i:
            scoped(f"absorb#i={i - 1}", absorb, *stages[i - 1])
        scoped(f"pass_on#i={i}", pass_on, *stages[i])
    for stage in behind + [stages[-1]]:
        scoped("absorb_last", absorb, *stage)

    fillers = []

    def blocks_of(body, steps, group):
        for start in range(0, steps, group):

            def run(start=start):
                def step(i, carry):
                    body(i)
                    return carry

                lax.fori_loop(start, min(start + group, steps), step, 0)

            fillers.append(run)

    wide = 256

    def gate_block(i):
        rows = r.slot_rows[:, span(i, wide)]
        r.gate_grad[0, span(i, wide), :] = dot(rows, r.d_gate[...], TN).astype(BF16)

    def up_block(i):
        rows = r.slot_rows[:, span(i, wide)]
        r.up_grad[0, span(i, wide), :] = dot(rows, r.d_up[...], TN).astype(BF16)

    def down_block(i):
        cols = span(i, wide)
        r.down_grad[0, :, cols] = dot(r.hidden[...], r.slot_cot[:, cols], TN).astype(BF16)

    blocks_of(down_block, full // wide, 2)
    blocks_of(gate_block, full // wide, 2)
    blocks_of(up_block, full // wide, 2)

    def fill(amount):
        for _ in range(amount):
            if fillers:
                scoped("fill", fillers.pop(0))

    halves = max(1, width // 128)
    half = width // halves
    order = list(range(deep - 1, -1, -1))
    core_copy, home_copy, line_copy = {}, {}, {}

    def kept_of(d, start, size):
        room = hidden_units // width
        first = d % room * width + start
        return (r.acc_gate, r.acc_up, r.acc_hidden)[d // room], slice(first, first + size)

    def pair_block(d):
        def chunk(rows):
            gate, up = r.d_gate[rows, :], r.d_up[rows, :]
            for which, block in enumerate((levels[d] * CORES + 1 - core, levels[d] * CORES + core)):
                value = dot(gate, r.wg[span(block, width), :], NT)
                value = value + dot(up, r.wu[span(block, width), :], NT)
                if which:
                    kept, cols = kept_of(d, 0, width)
                    kept[rows, cols] = value
                else:
                    r.stage[0, d, rows, :] = value.astype(BF16)

        row_loop(chunk)
        core_copy[d] = copies.start(r.stage.at[0, d], r.paired.at[d], partner)[1]

    def ship(d, h):
        if h == 0:
            core_copy[d].wait_recv()
        cols = slice(h * half, (h + 1) * half)
        kept, kept_cols = kept_of(d, h * half, half)
        joint = kept[:, kept_cols] + r.paired[d, :, cols].astype(F32)
        r.stage[1, d, :, cols] = joint.astype(BF16)
        for k in range(1, experts):
            home_copy[d, h, k] = copies.start(
                r.stage.at[1, d, span(planes[k][0], cap), pl.ds(h * half, half)],
                r.homed.at[h, d, span(sp, cap)],
                planes[k],
            )[1]
        r.homed[h, d, span(sp, cap), :] = r.stage[1, d, span(sp, cap), cols]

    def home(d, h):
        for k in range(1, experts):
            home_copy[d, h, k].wait_recv()
        summed = dot(r.taking[...], r.homed[h, d])
        if d:
            r.line_out[h, d - 1] = summed.astype(BF16)
            line_copy[d, h] = copies.start(
                r.line_out.at[h, d - 1], r.line_in.at[h, d - 1], lines[d]
            )[1]
        else:
            cols = slice(h * half, (h + 1) * half)
            r.sum_own[h] = summed + r.cot[:, cols].astype(F32)

    def spot_of(place_of, h):
        return r.block_grad.at[:, span(place_of * halves + h, half)]

    gathers, shared = {}, {}

    def close_sum(h):
        value = r.sum_own[h]
        for d in order[:-1]:
            line_copy[d, h].wait_recv()
            value = value + r.line_in[h, d - 1].astype(F32)
        r.block_grad[:, span(tp * halves + h, half)] = value.astype(BF16)
        spot = spot_of(tp, h)
        for d in range(1, deep):
            gathers[d, h] = copies.start(
                spot, spot, lines[d], middle if relay and d == 3 else None
            )
        shared[0, h] = copies.start(spot, spot, partner)[1]

    def gather(d, h):
        gathers[d, h][1].wait_recv()
        spot = spot_of(levels[d] * CORES + core, h)
        if relay and d == 2:
            copies.start(spot, spot, lines[1], middle, gathers[3, h][0])
        shared[d, h] = copies.start(spot, spot, partner)[1]

    share = (full // experts) // width
    pieces = {}

    def arrival_of(slot, q, h):
        return r.piece_sems.at[(slot * share + q) * halves + h]

    def use(d, h):
        shared[d, h].wait_recv()
        for c in range(CORES):
            block = levels[d] * CORES + c
            cols = span(block * halves + h, half)
            grads = r.block_grad[:, cols]
            value = dot(r.ow[:, cols], grads, NT)
            start = d == 0 and h == 0 and c == 0
            r.d_mixed[...] = value if start else r.d_mixed[...] + value
            r.product[d, h, c] = dot(r.mixed[...], grads).astype(BF16)
            to, q = lax.div(block, share), lax.rem(block, share)
            copy = pltpu.make_async_remote_copy(
                src_ref=r.product.at[d, h, c],
                dst_ref=r.products.at[sp, q, h],
                send_sem=r.sent_sems.at[(d * halves + h) * CORES + c],
                recv_sem=arrival_of(sp, q, h),
                device_id=(to, tp),
                device_id_type=pl.DeviceIdType.MESH,
            )
            pl.when(to != sp)(copy.start)
            copies.sent.append((to != sp, copy))

            @pl.when(to == sp)
            def _():
                r.products[sp, q, h] = r.product[d, h, c]

    with jax.named_scope("settle"):
        copies.finish()
    scoped("pair", pair_block, order[0])
    for i, d in enumerate(order):
        if i + 1 < deep:
            scoped("pair", pair_block, order[i + 1])
        scoped("ship", ship, d, 0)
    for h in range(1, halves):
        for d in order:
            scoped("ship", ship, d, h)
    for h in range(halves):
        for i, d in enumerate(order):
            fill(1)
            scoped(f"home#h={h}#d={d}", home, d, h)
            if h and i == 0:
                scoped("sum", close_sum, h - 1)
            if h and i == 2:
                scoped("gather", gather, 1, h - 1)
            if h and i == 3:
                scoped("gather", gather, 2, h - 1)
                for e in range(3, deep):
                    scoped("gather", gather, e, h - 1)
                for e in range(2):
                    scoped("use", use, e, h - 1)
    scoped("sum", close_sum, halves - 1)
    for h in range(halves - 1):
        for d in range(2, deep):
            scoped("use", use, d, h)
    fill(100)
    scoped("use", use, 0, halves - 1)
    for d in range(1, deep):
        scoped("gather", gather, d, halves - 1)
        if d > 1:
            scoped("use", use, d - 1, halves - 1)
    scoped("use", use, deep - 1, halves - 1)

    d_mixed = r.d_mixed[...]
    value = d_mixed * r.keep[4]
    reach, level = 1, 0
    while reach < length:
        value = value + r.reach[level] * pltpu.roll(value, length - reach, 1)
        reach *= 2
        level += 1
    decay_first = r.keep[5][:, 0:1]
    r.summary[0:1, :] = to_row(decay_first * r.keep[6][:, 0:1])
    r.summary[1:2, :] = to_row(decay_first * value[:, 0:1])
    tails = []
    for k in range(1, experts):
        tails.append(copies.start(r.summary, r.summaries.at[sp], planes[k])[1])
    r.summaries[sp] = r.summary[...]
    r.valve[...] = (d_mixed * r.keep[3]).astype(BF16)
    with jax.named_scope("summaries"):
        for copy in tails:
            copy.wait_recv()
    carried = jnp.zeros((1, channels), F32)
    for later in range(experts - 1, 0, -1):
        longer = r.summaries[later, 1:2, :] + r.summaries[later, 0:1, :] * carried
        carried = jnp.where(later > sp, longer, carried)
    state_grad = value + r.keep[6] * to_column(carried)
    grad_recur = (state_grad * r.keep[0]).astype(BF16)
    grad_input = (state_grad * r.keep[1]).astype(BF16)
    conv_grad = state_grad * r.keep[2]
    conv_grad = conv_grad + by_head(r.wr, grad_recur, NN) + by_head(r.wi, grad_input, NN)
    r.conv_grad[...] = conv_grad.astype(BF16)
    with jax.named_scope("products"):
        for k in range(1, experts):
            for q in range(share):
                for h in range(halves):
                    spot = r.products.at[planes[k][0], q, h]
                    pltpu.make_async_remote_copy(
                        src_ref=r.product.at[0, 0, 0],
                        dst_ref=spot,
                        send_sem=r.sent_sems.at[0],
                        recv_sem=arrival_of(planes[k][0], q, h),
                        device_id=planes[k],
                        device_id_type=pl.DeviceIdType.MESH,
                    ).wait_recv()
    for q in range(share):
        for h in range(halves):
            value = r.products[0, q, h].astype(F32)
            for e in range(1, experts):
                value = value + r.products[e, q, h].astype(F32)
            r.out_grad[:, q * width + h * half : q * width + (h + 1) * half] = value
    copies.finish()


def export_kernel(*refs):
    count = (len(refs) - 1) // 2
    copies = [
        pltpu.make_async_copy(refs[i], refs[count + i], refs[-1].at[i]) for i in range(count)
    ]
    for copy in copies:
        copy.start()
    for copy in copies:
        copy.wait()


def local(
    cotangent,
    block_input,
    routes,
    route_weights,
    gate_weight,
    up_weight,
    down_weight,
    out_weight,
    conv_out,
    gate_pre,
    prior_states,
    recur_weight,
    input_gate_matrix,
    decay_param,
    decay_jump,
):
    experts, columns = lax.axis_size("sp"), lax.axis_size("tp")
    deep = columns // CORES
    tokens, width = cotangent.shape
    cap = -(-(5 * tokens * TOP_K // (4 * experts)) // 16) * 16
    total = experts * cap
    full = width * columns
    units = gate_weight.shape[2]
    channels, length = conv_out.shape
    heads = channels // HEAD_DIM
    doublings = (length - 1).bit_length()
    halves = max(1, width // 128)
    half = width // halves
    share = (full // experts) // width
    copies = 2 * deep * (experts + 2) + deep + halves * deep * (experts + 4) + experts
    vmem = pltpu.VMEM
    scratch = dict(
        rows=vmem((tokens, width), BF16),
        cot=vmem((tokens, width), BF16),
        wg=vmem((full, units), BF16),
        wu=vmem((full, units), BF16),
        wd=vmem((units, full), BF16),
        ow=vmem((channels, full), BF16),
        conv=vmem((channels, length), BF16),
        pre=vmem((channels, length), BF16),
        prior=vmem((channels, length), BF16),
        jump=vmem((channels, length), F32),
        wr=vmem((heads, HEAD_DIM, HEAD_DIM), BF16),
        wi=vmem((heads, HEAD_DIM, HEAD_DIM), BF16),
        held=vmem((2, deep - 1, tokens, width), BF16),
        placing=vmem((total, tokens), BF16),
        taking=vmem((tokens, total), BF16),
        slot_weight=vmem((total, 1), F32),
        stage=vmem((2, deep, total, width), BF16),
        slot_rows=vmem((total, full), BF16),
        slot_cot=vmem((total, full), BF16),
        acc_gate=vmem((total, units), F32),
        acc_up=vmem((total, units), F32),
        acc_hidden=vmem((total, units), F32),
        hidden=vmem((total, units), BF16),
        d_gate=vmem((total, units), BF16),
        d_up=vmem((total, units), BF16),
        paired=vmem((deep, total, width), BF16),
        homed=vmem((halves, deep, total, half), BF16),
        line_out=vmem((halves, deep - 1, tokens, half), BF16),
        line_in=vmem((halves, deep - 1, tokens, half), BF16),
        sum_own=vmem((halves, tokens, half), F32),
        block_grad=vmem((tokens, full), BF16),
        mixed=vmem((channels, length), BF16),
        d_mixed=vmem((channels, length), F32),
        keep=vmem((7, channels, length), F32),
        reach=vmem((doublings, channels, length), F32),
        product=vmem((deep, halves, CORES, channels, half), BF16),
        products=vmem((experts, share, halves, channels, half), BF16),
        summary=vmem((8, channels), F32),
        summaries=vmem((experts, 8, channels), F32),
        send_sems=pltpu.SemaphoreType.DMA((copies,)),
        recv_sems=pltpu.SemaphoreType.DMA((copies,)),
        local_sems=pltpu.SemaphoreType.DMA((12,)),
        sent_sems=pltpu.SemaphoreType.DMA((deep * halves * CORES,)),
        piece_sems=pltpu.SemaphoreType.DMA((experts * share * halves,)),
    )
    on_chip = pl.BlockSpec(memory_space=pltpu.VMEM)
    far = pl.BlockSpec(memory_space=pltpu.HBM)
    given = ("routes", "route_w", "rate")

    def in_hbm(x):
        return pltpu.with_memory_space_constraint(x, pltpu.HBM)

    results = pl.pallas_call(
        functools.partial(kernel, INPUTS + OUTPUTS + tuple(scratch), experts, deep, cap),
        out_shape=(
            vmem(gate_weight.shape, BF16),
            vmem(up_weight.shape, BF16),
            vmem(down_weight.shape, BF16),
            vmem((channels, full // experts), F32),
            vmem((channels, length), BF16),
            vmem((channels, length), BF16),
        ),
        in_specs=[on_chip if name in given else far for name in INPUTS],
        out_specs=(on_chip,) * 6,
        scratch_shapes=list(scratch.values()),
        compiler_params=pltpu.CompilerParams(
            collective_id=0, has_side_effects=True, vmem_limit_bytes=50 << 20
        ),
    )(
        in_hbm(block_input),
        in_hbm(cotangent),
        jnp.transpose(routes),
        jnp.transpose(route_weights),
        in_hbm(gate_weight),
        in_hbm(up_weight),
        in_hbm(down_weight),
        in_hbm(out_weight),
        in_hbm(conv_out),
        in_hbm(gate_pre),
        in_hbm(prior_states),
        in_hbm(recur_weight),
        in_hbm(input_gate_matrix),
        decay_param.reshape(columns, channels),
        in_hbm(decay_jump),
    )
    return pl.pallas_call(
        export_kernel,
        out_shape=[jax.ShapeDtypeStruct(x.shape, x.dtype) for x in results],
        in_specs=[on_chip] * len(results),
        out_specs=[far] * len(results),
        scratch_shapes=[pltpu.SemaphoreType.DMA((len(results),))],
        compiler_params=pltpu.CompilerParams(vmem_limit_bytes=1 << 20),
    )(*results)


def solution(mesh):
    in_specs = (
        P("sp", "tp"),
        P("sp", "tp"),
        P("sp", None),
        P("sp", None),
        P("sp", None, "tp"),
        P("sp", None, "tp"),
        P("sp", "tp", None),
        P("tp", None),
        P("tp", "sp"),
        P("tp", "sp"),
        P("tp", "sp"),
        P(),
        P(),
        P(),
        P("tp", "sp"),
    )
    out_specs = (
        P("sp", None, "tp"),
        P("sp", None, "tp"),
        P("sp", "tp", None),
        P("tp", "sp"),
        P("tp", "sp"),
        P("tp", "sp"),
    )
    return jax.shard_map(local, mesh=mesh, in_specs=in_specs, out_specs=out_specs, check_vma=False)
```

```python
import functools

import jax
import jax.numpy as jnp
from jax import lax
from jax.experimental import pallas as pl
from jax.experimental.pallas import tpu as pltpu
from jax.sharding import PartitionSpec as P

HEAD_DIM = 64
TOP_K = 2
RATE_SCALE = 8.0
CORES = 2
NN = (((1,), (0,)), ((), ()))
NT = (((1,), (1,)), ((), ()))
TN = (((0,), (0,)), ((), ()))
F32 = jnp.float32
BF16 = jnp.bfloat16


def dot(a, b, dims=NN):
    return lax.dot_general(a, b, dims, preferred_element_type=F32)


def across(place, step, size):
    result, bit = 0, 1
    while bit < size:
        result = result + lax.rem(lax.div(place, bit) + (step // bit) % 2, 2) * bit
        bit *= 2
    return result


def span(block, width):
    return pl.ds(pl.multiple_of(block * width, width), width)


def signal(devices):
    barrier = pltpu.get_barrier_semaphore()
    for device in devices:
        pl.semaphore_signal(
            barrier, inc=1, device_id=device, device_id_type=pl.DeviceIdType.MESH
        )


def log1p_small(y):
    series = y * (1.0 + y * (-0.5 + y * (1.0 / 3 + y * (-0.25 + y * (0.2 - y / 6.0)))))
    return jnp.where(y < 0.03125, series, jnp.log(1.0 + y))


def expm1_neg(x):
    series = 1.0 / 40320 * x + 1.0 / 5040
    for factor in (720, 120, 24, 6, 2):
        series = series * x + 1.0 / factor
    series = x * (series * x + 1.0)
    return jnp.where(x > -0.35, series, jnp.exp(x) - 1.0)


class Copies:
    def __init__(self, send_sems, recv_sems):
        self.sems = (send_sems, recv_sems)
        self.count = 0
        self.sent = []

    def start(self, source, target, device, when=None, arrival=None):
        index, self.count = self.count, self.count + 1
        copy = pltpu.make_async_remote_copy(
            src_ref=source,
            dst_ref=target,
            send_sem=self.sems[0].at[index],
            recv_sem=self.sems[1].at[index if arrival is None else arrival],
            device_id=device,
            device_id_type=pl.DeviceIdType.MESH,
        )
        self.run(when, copy.start)
        self.sent.append((when, copy))
        return index, copy

    def run(self, when, action):
        if when is None:
            action()
        else:
            pl.when(when)(action)

    def finish(self, amount=None):
        amount = len(self.sent) if amount is None else amount
        for when, copy in self.sent[:amount]:
            self.run(when, copy.wait_send)
        self.sent = self.sent[amount:]


INPUTS = (
    "rows_hbm", "cot_hbm", "routes", "route_w", "wg_hbm", "wu_hbm", "wd_hbm", "ow_hbm",
    "conv_hbm", "pre_hbm", "prior_hbm", "wr_hbm", "wi_hbm", "rate", "jump_hbm",
)
OUTPUTS = ("gate_grad", "down_grad", "out_grad", "conv_grad", "valve", "slot_rows", "d_up")


class Refs:
    pass


def kernel(names, experts, deep, cap, *refs):
    r = Refs()
    for name, ref in zip(names, refs):
        setattr(r, name, ref)
    sp, tp = lax.axis_index("sp"), lax.axis_index("tp")
    z, core = lax.div(tp, CORES), lax.rem(tp, CORES)
    partner = (sp, z * CORES + 1 - core)
    planes = [(across(sp, k, experts), tp) for k in range(experts)]
    levels = [across(z, d, deep) for d in range(deep)]
    lines = [(sp, level * CORES + core) for level in levels]
    tokens, width = r.rows.shape
    pair = CORES * width
    full = width * CORES * deep
    total = experts * cap
    hidden_units = r.wg.shape[1]
    channels, length = r.conv.shape
    heads = channels // HEAD_DIM
    copies = Copies(r.send_sems, r.recv_sems)
    sources = [
        (r.rows_hbm, r.rows), (r.cot_hbm, r.cot), (r.wg_hbm.at[0], r.wg),
        (r.wu_hbm.at[0], r.wu), (r.wd_hbm.at[0], r.wd), (r.conv_hbm, r.conv),
        (r.pre_hbm, r.pre), (r.prior_hbm, r.prior), (r.jump_hbm, r.jump),
        (r.wr_hbm.at[span(tp, heads)], r.wr), (r.wi_hbm.at[span(tp, heads)], r.wi),
        (r.ow_hbm, r.ow),
    ]
    local = [
        pltpu.make_async_copy(a, b, r.local_sems.at[i]) for i, (a, b) in enumerate(sources)
    ]
    peers = planes[1:] + lines[1:] + [partner]
    signal(peers)
    for copy in local:
        copy.start()
    with jax.named_scope("greet"):
        pl.semaphore_wait(pltpu.get_barrier_semaphore(), len(peers))
    local[0].wait()
    local[1].wait()
    own = (r.rows, r.cot)
    relieved = (1, 1)
    relay = deep == 4
    middle = (z == 1) | (z == 2)
    line = {}
    raw = [(a, d) for a in range(2) for d in range(1, deep) if (a, d) != relieved]
    for a, d in raw:
        line[a, d] = copies.start(
            own[a], r.held.at[a, d - 1], lines[d], middle if relay and d == 3 else None
        )

    expert_ids = lax.broadcasted_iota(jnp.int32, (16, tokens), 0)
    first = r.routes[0:1, :] == expert_ids
    second = r.routes[1:2, :] == expert_ids
    member = (first | second).astype(F32)
    weight_of = jnp.where(first, r.route_w[0:1, :], 0.0) + jnp.where(
        second, r.route_w[1:2, :], 0.0
    )
    earlier = lax.broadcasted_iota(jnp.int32, (tokens, tokens), 0) < lax.broadcasted_iota(
        jnp.int32, (tokens, tokens), 1
    )
    rank = dot(member.astype(BF16), earlier.astype(F32).astype(BF16))
    rank = jnp.where(member > 0.5, rank, -1.0)
    slot_ids = lax.broadcasted_iota(jnp.int32, (cap, tokens), 0).astype(F32)
    for e in range(experts):
        hit = slot_ids == rank[e : e + 1, :]
        r.placing[e * cap : (e + 1) * cap, :] = jnp.where(hit, 1.0, 0.0).astype(BF16)
        r.slot_weight[e * cap : (e + 1) * cap, :] = jnp.sum(
            jnp.where(hit, weight_of[e : e + 1, :], 0.0), axis=1, keepdims=True
        )

    filled = (r.slot_rows, r.slot_cot)
    plane, forward = {}, {}

    def here_of(d):
        return span(levels[d] * CORES + core, width)

    def issue(a, d):
        if d:
            line[a, d][1].wait_recv()
        if relay and d == 2:
            copies.start(
                r.held.at[a, 1], r.held.at[a, 2], lines[1], middle, line[a, 3][0]
            )
        block = r.held[a, d - 1] if d else own[a][...]
        placed = dot(r.placing[...], block)
        if a:
            placed = placed * r.slot_weight[...]
        r.stage[a, d] = placed.astype(BF16)
        for k in range(1, experts):
            plane[a, d, k] = copies.start(
                r.stage.at[a, d, span(planes[k][0], cap)],
                filled[a].at[span(sp, cap), here_of(d)],
                planes[k],
            )[1]
        filled[a][span(sp, cap), here_of(d)] = r.stage[a, d, span(sp, cap), :]

    def pass_on(a, d):
        if (a, d) == relieved:
            line[a, d].wait_recv()
        else:
            for k in range(1, experts):
                plane[a, d, k].wait_recv()
        here = filled[a].at[:, here_of(d)]
        forward[a, d] = copies.start(here, here, partner)[1]

    def relieve():
        there = filled[relieved[0]].at[:, here_of(0)]
        line[relieved] = copies.start(there, there, lines[relieved[1]])[1]

    def row_loop(body):
        size = total // 2

        def step(i, carry):
            body(span(i, size))
            return carry

        lax.fori_loop(0, 2, step, 0)

    seen = [0, 0]

    def absorb(a, d):
        forward[a, d].wait_recv()
        cols = span(levels[d], pair)
        order = seen[a]
        seen[a] += 1
        if a == 0:
            if order == 0:
                local[2].wait()
                local[3].wait()

            def chunk(rows):
                x = r.slot_rows[rows, cols]
                gate = dot(x, r.wg[cols, :])
                up = dot(x, r.wu[cols, :])
                if order:
                    gate = gate + r.acc_gate[rows, :]
                    up = up + r.acc_up[rows, :]
                if order == deep - 1:
                    sigma = jax.nn.sigmoid(gate)
                    silu = gate * sigma
                    r.hidden[rows, :] = (silu * up).astype(BF16)
                    gate = up * (sigma * (1.0 + gate * (1.0 - sigma)))
                    up = silu
                r.acc_gate[rows, :] = gate
                r.acc_up[rows, :] = up
        else:
            if order == 0:
                local[4].wait()

            def chunk(rows):
                value = dot(r.slot_cot[rows, cols], r.wd[:, cols], NT)
                if order:
                    value = value + r.acc_hidden[rows, :]
                if order < deep - 1:
                    r.acc_hidden[rows, :] = value
                else:
                    r.d_gate[rows, :] = (value * r.acc_gate[rows, :]).astype(BF16)
                    r.d_up[rows, :] = (value * r.acc_up[rows, :]).astype(BF16)

        row_loop(chunk)

    eye = lax.broadcasted_iota(jnp.int32, (channels, channels), 0) == lax.broadcasted_iota(
        jnp.int32, (channels, channels), 1
    )
    place = lax.broadcasted_iota(jnp.int32, (channels, length), 1)

    def to_column(row):
        return jnp.sum(jnp.where(eye, row, 0.0), axis=1, keepdims=True)

    def to_row(column):
        return jnp.sum(jnp.where(eye, column, 0.0), axis=0, keepdims=True)

    def by_head(weights, x, dims):
        return jnp.concatenate(
            [
                dot(weights[h], x[h * HEAD_DIM : (h + 1) * HEAD_DIM, :], dims)
                for h in range(heads)
            ],
            axis=0,
        )

    def prepare_gates():
        for i in range(5, 12):
            local[i].wait()
        conv = r.conv[...].astype(F32)
        prior = r.prior[...].astype(F32)
        recur = jax.nn.sigmoid(by_head(r.wr, r.conv[...], TN))
        gate = jax.nn.sigmoid(by_head(r.wi, r.conv[...], TN))
        rate = -r.rate[pl.ds(tp, 1), :]
        soft = to_column(jnp.maximum(rate, 0.0) + log1p_small(jnp.exp(-jnp.abs(rate))))
        log_decay = -RATE_SCALE * recur * soft + r.jump[...]
        decay = jnp.exp(log_decay)
        norm = jnp.sqrt(-expm1_neg(2.0 * log_decay))
        state = decay * prior + norm * gate * conv
        x = r.pre[...].astype(F32)
        inner = 0.7978845608028654 * (x + 0.044715 * (x * x * x))
        bend = jnp.tanh(inner)
        gelu = 0.5 * x * (1.0 + bend)
        slope = 0.5 * (1.0 + bend) + 0.5 * x * (1.0 - bend * bend) * (
            0.7978845608028654 * (1.0 + 3 * 0.044715 * (x * x))
        )
        r.mixed[...] = (gelu * state).astype(BF16)
        pull = prior * decay - gate * conv * decay * decay / norm
        r.keep[0] = pull * (-RATE_SCALE * soft) * recur * (1.0 - recur)
        r.keep[1] = norm * conv * gate * (1.0 - gate)
        r.keep[2] = norm * gate
        r.keep[3] = slope * state
        r.keep[4] = gelu
        r.keep[5] = decay

    def prepare_scan():
        decay = r.keep[5]
        later = jnp.where(place < length - 1, pltpu.roll(decay, length - 1, 1), 1.0)
        reach, level = 1, 0
        while reach < length:
            inside = place < length - reach
            r.reach[level] = jnp.where(inside, later, 0.0)
            later = later * jnp.where(inside, pltpu.roll(later, length - reach, 1), 1.0)
            reach *= 2
            level += 1
        r.keep[6] = later

    def prepare_taking():
        r.taking[...] = r.placing[...].T

    def scoped(name, fn, *args):
        with jax.named_scope(name):
            fn(*args)

    stages = [(0, 0), (1, 0)] + [(0, d) for d in range(1, deep)]
    stages += [(1, d) for d in range(2, deep)]
    between = {0: prepare_gates, 1: prepare_scan, 2: prepare_taking}
    scoped("issue", issue, *stages[0])
    scoped("issue", issue, *stages[1])
    count = len(stages)
    behind = []
    for i in range(count):
        if i in between:
            scoped("between", between[i])
        if i + 2 < count:
            scoped(f"issue#i={i + 2}", issue, *stages[i + 2])
        if i + 2 == count - 1 - (deep - 1 > 2):
            relieve()
        if i == count - 1:
            scoped("pass_on_relieved", pass_on, *relieved)
            scoped("absorb_relieved", absorb, *stages[i - 1])
            behind = [relieved]
        elif i:
            scoped(f"absorb#i={i - 1}", absorb, *stages[i - 1])
        scoped(f"pass_on#i={i}", pass_on, *stages[i])
    for stage in behind + [stages[-1]]:
        scoped("absorb_last", absorb, *stage)

    fillers = []

    def blocks_of(body, steps, group):
        for start in range(0, steps, group):

            def run(start=start):
                def step(i, carry):
                    body(i)
                    return carry

                lax.fori_loop(start, min(start + group, steps), step, 0)

            fillers.append(run)

    wide = 256

    def gate_block(i):
        rows = r.slot_rows[:, span(i, wide)]
        r.gate_grad[0, span(i, wide), :] = dot(rows, r.d_gate[...], TN).astype(BF16)

    def down_block(i):
        cols = span(i, wide)
        r.down_grad[0, :, cols] = dot(r.hidden[...], r.slot_cot[:, cols], TN).astype(BF16)

    blocks_of(down_block, full // wide, 2)
    blocks_of(gate_block, full // wide, 2)

    def fill(amount):
        for _ in range(amount):
            if fillers:
                scoped("fill", fillers.pop(0))

    halves = max(1, width // 128)
    half = width // halves
    order = list(range(deep - 1, -1, -1))
    core_copy, home_copy, line_copy = {}, {}, {}

    def kept_of(d, start, size):
        room = hidden_units // width
        first = d % room * width + start
        return (r.acc_gate, r.acc_up, r.acc_hidden)[d // room], slice(first, first + size)

    def pair_block(d):
        def chunk(rows):
            gate, up = r.d_gate[rows, :], r.d_up[rows, :]
            for which, block in enumerate((levels[d] * CORES + 1 - core, levels[d] * CORES + core)):
                value = dot(gate, r.wg[span(block, width), :], NT)
                value = value + dot(up, r.wu[span(block, width), :], NT)
                if which:
                    kept, cols = kept_of(d, 0, width)
                    kept[rows, cols] = value
                else:
                    r.stage[0, d, rows, :] = value.astype(BF16)

        row_loop(chunk)
        core_copy[d] = copies.start(r.stage.at[0, d], r.paired.at[d], partner)[1]

    def ship(d, h):
        if h == 0:
            core_copy[d].wait_recv()
        cols = slice(h * half, (h + 1) * half)
        kept, kept_cols = kept_of(d, h * half, half)
        joint = kept[:, kept_cols] + r.paired[d, :, cols].astype(F32)
        r.stage[1, d, :, cols] = joint.astype(BF16)
        for k in range(1, experts):
            home_copy[d, h, k] = copies.start(
                r.stage.at[1, d, span(planes[k][0], cap), pl.ds(h * half, half)],
                r.homed.at[h, d, span(sp, cap)],
                planes[k],
            )[1]
        r.homed[h, d, span(sp, cap), :] = r.stage[1, d, span(sp, cap), cols]

    def home(d, h):
        for k in range(1, experts):
            home_copy[d, h, k].wait_recv()
        summed = dot(r.taking[...], r.homed[h, d])
        if d:
            r.line_out[h, d - 1] = summed.astype(BF16)
            line_copy[d, h] = copies.start(
                r.line_out.at[h, d - 1], r.line_in.at[h, d - 1], lines[d]
            )[1]
        else:
            cols = slice(h * half, (h + 1) * half)
            r.sum_own[h] = summed + r.cot[:, cols].astype(F32)

    def spot_of(place_of, h):
        return r.block_grad.at[:, span(place_of * halves + h, half)]

    gathers, shared = {}, {}

    def close_sum(h):
        value = r.sum_own[h]
        for d in order[:-1]:
            line_copy[d, h].wait_recv()
            value = value + r.line_in[h, d - 1].astype(F32)
        r.block_grad[:, span(tp * halves + h, half)] = value.astype(BF16)
        spot = spot_of(tp, h)
        for d in range(1, deep):
            gathers[d, h] = copies.start(
                spot, spot, lines[d], middle if relay and d == 3 else None
            )
        shared[0, h] = copies.start(spot, spot, partner)[1]

    def gather(d, h):
        gathers[d, h][1].wait_recv()
        spot = spot_of(levels[d] * CORES + core, h)
        if relay and d == 2:
            copies.start(spot, spot, lines[1], middle, gathers[3, h][0])
        shared[d, h] = copies.start(spot, spot, partner)[1]

    share = (full // experts) // width
    pieces = {}

    def arrival_of(slot, q, h):
        return r.piece_sems.at[(slot * share + q) * halves + h]

    def use(d, h):
        mix(d, h)
        spread(d, h)

    def mix(d, h):
        shared[d, h].wait_recv()
        value = None if d == 0 and h == 0 else r.d_mixed[...]
        for c in range(CORES):
            cols = span((levels[d] * CORES + c) * halves + h, half)
            part = dot(r.ow[:, cols], r.block_grad[:, cols], NT)
            value = part if value is None else value + part
        r.d_mixed[...] = value

    def spread(d, h):
        for c in range(CORES):
            block = levels[d] * CORES + c
            grads = r.block_grad[:, span(block * halves + h, half)]
            r.product[d, h, c] = dot(r.mixed[...], grads).astype(BF16)
            to, q = lax.div(block, share), lax.rem(block, share)
            copy = pltpu.make_async_remote_copy(
                src_ref=r.product.at[d, h, c],
                dst_ref=r.products.at[sp, q, h],
                send_sem=r.sent_sems.at[(d * halves + h) * CORES + c],
                recv_sem=arrival_of(sp, q, h),
                device_id=(to, tp),
                device_id_type=pl.DeviceIdType.MESH,
            )
            pl.when(to != sp)(copy.start)
            copies.sent.append((to != sp, copy))

            @pl.when(to == sp)
            def _():
                r.products[sp, q, h] = r.product[d, h, c]

    with jax.named_scope("settle"):
        copies.finish()
    scoped("pair", pair_block, order[0])
    for i, d in enumerate(order):
        if i + 1 < deep:
            scoped("pair", pair_block, order[i + 1])
        scoped("ship", ship, d, 0)
    for h in range(1, halves):
        for d in order:
            scoped("ship", ship, d, h)
    for h in range(halves):
        for i, d in enumerate(order):
            fill(1)
            scoped(f"home#h={h}#d={d}", home, d, h)
            if h and i == 0:
                scoped("sum", close_sum, h - 1)
            if h and i == 2:
                fill(1)
                scoped("gather", gather, 1, h - 1)
            if h and i == 3:
                fill(1)
                scoped("gather", gather, 2, h - 1)
                for e in range(3, deep):
                    scoped("gather", gather, e, h - 1)
                for e in range(2):
                    scoped("use", use, e, h - 1)
    scoped("sum", close_sum, halves - 1)
    for h in range(halves - 1):
        for d in range(2, deep):
            scoped("use", use, d, h)
    fill(100)
    scoped("use", use, 0, halves - 1)
    for d in range(1, deep):
        scoped("gather", gather, d, halves - 1)
        if d > 1:
            scoped("mix", mix, d - 1, halves - 1)
        if d == 2:
            scoped("spread", spread, 1, halves - 1)
    scoped("mix", mix, deep - 1, halves - 1)

    d_mixed = r.d_mixed[...]
    value = d_mixed * r.keep[4]
    reach, level = 1, 0
    while reach < length:
        value = value + r.reach[level] * pltpu.roll(value, length - reach, 1)
        reach *= 2
        level += 1
    decay_first = r.keep[5][:, 0:1]
    r.summary[0:1, :] = to_row(decay_first * r.keep[6][:, 0:1])
    r.summary[1:2, :] = to_row(decay_first * value[:, 0:1])
    tails = []
    for k in range(1, experts):
        tails.append(copies.start(r.summary, r.summaries.at[sp], planes[k])[1])
    r.summaries[sp] = r.summary[...]
    r.valve[...] = (d_mixed * r.keep[3]).astype(BF16)
    for d in range(2, deep):
        scoped("spread", spread, d, halves - 1)
    with jax.named_scope("settle"):
        copies.finish(len(copies.sent) - (deep - 2) * CORES - experts)
    with jax.named_scope("summaries"):
        for copy in tails:
            copy.wait_recv()
    carried = jnp.zeros((1, channels), F32)
    for later in range(experts - 1, 0, -1):
        longer = r.summaries[later, 1:2, :] + r.summaries[later, 0:1, :] * carried
        carried = jnp.where(later > sp, longer, carried)
    state_grad = value + r.keep[6] * to_column(carried)
    grad_recur = (state_grad * r.keep[0]).astype(BF16)
    grad_input = (state_grad * r.keep[1]).astype(BF16)
    conv_grad = state_grad * r.keep[2]
    conv_grad = conv_grad + by_head(r.wr, grad_recur, NN) + by_head(r.wi, grad_input, NN)
    r.conv_grad[...] = conv_grad.astype(BF16)
    with jax.named_scope("products"):
        for k in range(1, experts):
            for q in range(share):
                for h in range(halves):
                    spot = r.products.at[planes[k][0], q, h]
                    pltpu.make_async_remote_copy(
                        src_ref=r.product.at[0, 0, 0],
                        dst_ref=spot,
                        send_sem=r.sent_sems.at[0],
                        recv_sem=arrival_of(planes[k][0], q, h),
                        device_id=planes[k],
                        device_id_type=pl.DeviceIdType.MESH,
                    ).wait_recv()
    for q in range(share):
        for h in range(halves):
            value = r.products[0, q, h].astype(F32)
            for e in range(1, experts):
                value = value + r.products[e, q, h].astype(F32)
            r.out_grad[:, q * width + h * half : q * width + (h + 1) * half] = value
    copies.finish()


def export_kernel(gate, down, out, conv, valve, rows, d_up, *refs):
    outs, (block, sems, up_sems) = refs[:6], refs[6:]
    whole = [
        pltpu.make_async_copy(a, b, sems.at[i])
        for i, (a, b) in enumerate(zip((gate, down, out, conv, valve), outs))
    ]
    for copy in whole:
        copy.start()
    wide = block.shape[1]
    steps = rows.shape[1] // wide
    pieces = []
    for i in range(steps):
        part = pl.ds(i * wide, wide)
        block[i] = dot(rows[:, part], d_up[...], TN).astype(BF16)
        pieces.append(
            pltpu.make_async_copy(block.at[i], outs[5].at[0, part, :], up_sems.at[i])
        )
        pieces[-1].start()
    for copy in whole + pieces:
        copy.wait()


def local(
    cotangent,
    block_input,
    routes,
    route_weights,
    gate_weight,
    up_weight,
    down_weight,
    out_weight,
    conv_out,
    gate_pre,
    prior_states,
    recur_weight,
    input_gate_matrix,
    decay_param,
    decay_jump,
):
    experts, columns = lax.axis_size("sp"), lax.axis_size("tp")
    deep = columns // CORES
    tokens, width = cotangent.shape
    cap = -(-(5 * tokens * TOP_K // (4 * experts)) // 16) * 16
    total = experts * cap
    full = width * columns
    units = gate_weight.shape[2]
    channels, length = conv_out.shape
    heads = channels // HEAD_DIM
    doublings = (length - 1).bit_length()
    halves = max(1, width // 128)
    half = width // halves
    share = (full // experts) // width
    copies = 2 * deep * (experts + 2) + deep + halves * deep * (experts + 4) + experts
    vmem = pltpu.VMEM
    scratch = dict(
        rows=vmem((tokens, width), BF16),
        cot=vmem((tokens, width), BF16),
        wg=vmem((full, units), BF16),
        wu=vmem((full, units), BF16),
        wd=vmem((units, full), BF16),
        ow=vmem((channels, full), BF16),
        conv=vmem((channels, length), BF16),
        pre=vmem((channels, length), BF16),
        prior=vmem((channels, length), BF16),
        jump=vmem((channels, length), F32),
        wr=vmem((heads, HEAD_DIM, HEAD_DIM), BF16),
        wi=vmem((heads, HEAD_DIM, HEAD_DIM), BF16),
        held=vmem((2, deep - 1, tokens, width), BF16),
        placing=vmem((total, tokens), BF16),
        taking=vmem((tokens, total), BF16),
        slot_weight=vmem((total, 1), F32),
        stage=vmem((2, deep, total, width), BF16),
        slot_cot=vmem((total, full), BF16),
        acc_gate=vmem((total, units), F32),
        acc_up=vmem((total, units), F32),
        acc_hidden=vmem((total, units), F32),
        hidden=vmem((total, units), BF16),
        d_gate=vmem((total, units), BF16),
        paired=vmem((deep, total, width), BF16),
        homed=vmem((halves, deep, total, half), BF16),
        line_out=vmem((halves, deep - 1, tokens, half), BF16),
        line_in=vmem((halves, deep - 1, tokens, half), BF16),
        sum_own=vmem((halves, tokens, half), F32),
        block_grad=vmem((tokens, full), BF16),
        mixed=vmem((channels, length), BF16),
        d_mixed=vmem((channels, length), F32),
        keep=vmem((7, channels, length), F32),
        reach=vmem((doublings, channels, length), F32),
        product=vmem((deep, halves, CORES, channels, half), BF16),
        products=vmem((experts, share, halves, channels, half), BF16),
        summary=vmem((8, channels), F32),
        summaries=vmem((experts, 8, channels), F32),
        send_sems=pltpu.SemaphoreType.DMA((copies,)),
        recv_sems=pltpu.SemaphoreType.DMA((copies,)),
        local_sems=pltpu.SemaphoreType.DMA((12,)),
        sent_sems=pltpu.SemaphoreType.DMA((deep * halves * CORES,)),
        piece_sems=pltpu.SemaphoreType.DMA((experts * share * halves,)),
    )
    on_chip = pl.BlockSpec(memory_space=pltpu.VMEM)
    far = pl.BlockSpec(memory_space=pltpu.HBM)
    given = ("routes", "route_w", "rate")

    def in_hbm(x):
        return pltpu.with_memory_space_constraint(x, pltpu.HBM)

    results = pl.pallas_call(
        functools.partial(kernel, INPUTS + OUTPUTS + tuple(scratch), experts, deep, cap),
        out_shape=(
            vmem(gate_weight.shape, BF16),
            vmem(down_weight.shape, BF16),
            vmem((channels, full // experts), F32),
            vmem((channels, length), BF16),
            vmem((channels, length), BF16),
            vmem((total, full), BF16),
            vmem((total, units), BF16),
        ),
        in_specs=[on_chip if name in given else far for name in INPUTS],
        out_specs=(on_chip,) * len(OUTPUTS),
        scratch_shapes=list(scratch.values()),
        compiler_params=pltpu.CompilerParams(
            collective_id=0, has_side_effects=True, vmem_limit_bytes=50 << 20
        ),
    )(
        in_hbm(block_input),
        in_hbm(cotangent),
        jnp.transpose(routes),
        jnp.transpose(route_weights),
        in_hbm(gate_weight),
        in_hbm(up_weight),
        in_hbm(down_weight),
        in_hbm(out_weight),
        in_hbm(conv_out),
        in_hbm(gate_pre),
        in_hbm(prior_states),
        in_hbm(recur_weight),
        in_hbm(input_gate_matrix),
        decay_param.reshape(columns, channels),
        in_hbm(decay_jump),
    )
    wide = 256
    saved = [jax.ShapeDtypeStruct(x.shape, x.dtype) for x in results[:5]]
    gate, down, out, conv, valve, up = pl.pallas_call(
        export_kernel,
        out_shape=saved + [jax.ShapeDtypeStruct(up_weight.shape, BF16)],
        in_specs=[on_chip] * len(results),
        out_specs=[far] * 6,
        scratch_shapes=[
            vmem((full // wide, wide, units), BF16),
            pltpu.SemaphoreType.DMA((5,)),
            pltpu.SemaphoreType.DMA((full // wide,)),
        ],
        compiler_params=pltpu.CompilerParams(vmem_limit_bytes=12 << 20),
    )(*results)
    return gate, up, down, out, conv, valve


def solution(mesh):
    in_specs = (
        P("sp", "tp"),
        P("sp", "tp"),
        P("sp", None),
        P("sp", None),
        P("sp", None, "tp"),
        P("sp", None, "tp"),
        P("sp", "tp", None),
        P("tp", None),
        P("tp", "sp"),
        P("tp", "sp"),
        P("tp", "sp"),
        P(),
        P(),
        P(),
        P("tp", "sp"),
    )
    out_specs = (
        P("sp", None, "tp"),
        P("sp", None, "tp"),
        P("sp", "tp", None),
        P("tp", "sp"),
        P("tp", "sp"),
        P("tp", "sp"),
    )
    return jax.shard_map(local, mesh=mesh, in_specs=in_specs, out_specs=out_specs, check_vma=False)
```

```python
import functools

import jax
import jax.numpy as jnp
from jax import lax
from jax.experimental import pallas as pl
from jax.experimental.pallas import tpu as pltpu
from jax.sharding import PartitionSpec as P

HEAD_DIM = 64
TOP_K = 2
RATE_SCALE = 8.0
CORES = 2
NN = (((1,), (0,)), ((), ()))
NT = (((1,), (1,)), ((), ()))
TN = (((0,), (0,)), ((), ()))
F32 = jnp.float32
BF16 = jnp.bfloat16


def dot(a, b, dims=NN):
    return lax.dot_general(a, b, dims, preferred_element_type=F32)


def across(place, step, size):
    result, bit = 0, 1
    while bit < size:
        result = result + lax.rem(lax.div(place, bit) + (step // bit) % 2, 2) * bit
        bit *= 2
    return result


def span(block, width):
    return pl.ds(pl.multiple_of(block * width, width), width)


def signal(devices):
    barrier = pltpu.get_barrier_semaphore()
    for device in devices:
        pl.semaphore_signal(
            barrier, inc=1, device_id=device, device_id_type=pl.DeviceIdType.MESH
        )


def log1p_small(y):
    series = y * (1.0 + y * (-0.5 + y * (1.0 / 3 + y * (-0.25 + y * (0.2 - y / 6.0)))))
    return jnp.where(y < 0.03125, series, jnp.log(1.0 + y))


def expm1_neg(x):
    series = 1.0 / 40320 * x + 1.0 / 5040
    for factor in (720, 120, 24, 6, 2):
        series = series * x + 1.0 / factor
    series = x * (series * x + 1.0)
    return jnp.where(x > -0.35, series, jnp.exp(x) - 1.0)


class Copies:
    def __init__(self, send_sems, recv_sems):
        self.sems = (send_sems, recv_sems)
        self.sends, self.arrivals, self.count = 0, 0, 0
        self.sent = []

    def make(self, source, target, device, send, arrival):
        return pltpu.make_async_remote_copy(
            src_ref=source,
            dst_ref=target,
            send_sem=self.sems[0].at[send],
            recv_sem=self.sems[1].at[arrival],
            device_id=device,
            device_id_type=pl.DeviceIdType.MESH,
        )

    def take_send(self):
        send, self.sends = self.sends, self.sends + 1
        self.count = max(self.count, self.sends)
        assert self.sends <= self.sems[0].shape[0]
        return send

    def take_arrival(self):
        arrival, self.arrivals = self.arrivals, self.arrivals + 1
        assert self.arrivals <= self.sems[1].shape[0]
        return arrival

    def start(self, source, target, device, when=None, arrival=None):
        arrival = self.take_arrival() if arrival is None else arrival
        copy = self.make(source, target, device, self.take_send(), arrival)
        self.run(when, copy.start)
        self.sent.append((when, copy))
        return arrival, copy

    def start_all(self, pairs, sent, landed, device):
        send, arrival = self.take_send(), self.take_arrival()
        for source, target, to in pairs:
            self.make(source, target, to, send, arrival).start()
        copy = self.make(sent, landed, device, send, arrival)
        self.sent.append((None, copy))
        return copy

    def run(self, when, action):
        if when is None:
            action()
        else:
            pl.when(when)(action)

    def finish(self, amount=None):
        amount = len(self.sent) if amount is None else amount
        for when, copy in self.sent[:amount]:
            self.run(when, copy.wait_send)
        self.sent = self.sent[amount:]
        if not self.sent:
            self.sends = 0


INPUTS = (
    "rows_hbm", "cot_hbm", "routes", "route_w", "wg_hbm", "wu_hbm", "wd_hbm", "ow_hbm",
    "conv_hbm", "pre_hbm", "prior_hbm", "wr_hbm", "wi_hbm", "rate", "jump_hbm",
)
OUTPUTS = ("gate_grad", "down_grad", "out_grad", "conv_grad", "valve", "slot_rows", "d_up")


class Refs:
    pass


def kernel(names, experts, deep, cap, *refs):
    r = Refs()
    for name, ref in zip(names, refs):
        setattr(r, name, ref)
    sp, tp = lax.axis_index("sp"), lax.axis_index("tp")
    z, core = lax.div(tp, CORES), lax.rem(tp, CORES)
    partner = (sp, z * CORES + 1 - core)
    planes = [(across(sp, k, experts), tp) for k in range(experts)]
    levels = [across(z, d, deep) for d in range(deep)]
    lines = [(sp, level * CORES + core) for level in levels]
    tokens, width = r.rows.shape
    pair = CORES * width
    full = width * CORES * deep
    total = experts * cap
    hidden_units = r.wg.shape[1]
    channels, length = r.conv.shape
    heads = channels // HEAD_DIM
    copies = Copies(r.send_sems, r.recv_sems)
    sources = [
        (r.rows_hbm, r.rows), (r.cot_hbm, r.cot), (r.wg_hbm.at[0], r.wg),
        (r.wu_hbm.at[0], r.wu), (r.wd_hbm.at[0], r.wd), (r.conv_hbm, r.conv),
        (r.pre_hbm, r.pre), (r.prior_hbm, r.prior), (r.jump_hbm, r.jump),
        (r.wr_hbm.at[span(tp, heads)], r.wr), (r.wi_hbm.at[span(tp, heads)], r.wi),
        (r.ow_hbm, r.ow),
    ]
    local = [
        pltpu.make_async_copy(a, b, r.local_sems.at[i]) for i, (a, b) in enumerate(sources)
    ]
    peers = planes[1:] + lines[1:] + [partner]
    signal(peers)
    for copy in local:
        copy.start()
    with jax.named_scope("greet"):
        pl.semaphore_wait(pltpu.get_barrier_semaphore(), len(peers))
    local[0].wait()
    local[1].wait()
    own = (r.rows, r.cot)
    relieved = (1, 1)
    relay = deep == 4
    middle = (z == 1) | (z == 2)
    line = {}
    raw = [(a, d) for a in range(2) for d in range(1, deep) if (a, d) != relieved]
    for a, d in raw:
        line[a, d] = copies.start(
            own[a], r.held.at[a, d - 1], lines[d], middle if relay and d == 3 else None
        )

    expert_ids = lax.broadcasted_iota(jnp.int32, (16, tokens), 0)
    first = r.routes[0:1, :] == expert_ids
    second = r.routes[1:2, :] == expert_ids
    member = (first | second).astype(F32)
    weight_of = jnp.where(first, r.route_w[0:1, :], 0.0) + jnp.where(
        second, r.route_w[1:2, :], 0.0
    )
    earlier = lax.broadcasted_iota(jnp.int32, (tokens, tokens), 0) < lax.broadcasted_iota(
        jnp.int32, (tokens, tokens), 1
    )
    rank = dot(member.astype(BF16), earlier.astype(F32).astype(BF16))
    rank = jnp.where(member > 0.5, rank, -1.0)
    slot_ids = lax.broadcasted_iota(jnp.int32, (cap, tokens), 0).astype(F32)
    for e in range(experts):
        hit = slot_ids == rank[e : e + 1, :]
        r.placing[e * cap : (e + 1) * cap, :] = jnp.where(hit, 1.0, 0.0).astype(BF16)
        r.slot_weight[e * cap : (e + 1) * cap, :] = jnp.sum(
            jnp.where(hit, weight_of[e : e + 1, :], 0.0), axis=1, keepdims=True
        )

    filled = (r.slot_rows, r.slot_cot)
    plane, forward = {}, {}

    def here_of(d):
        return span(levels[d] * CORES + core, width)

    def issue(a, d):
        if d:
            line[a, d][1].wait_recv()
        if relay and d == 2:
            copies.start(
                r.held.at[a, 1], r.held.at[a, 2], lines[1], middle, line[a, 3][0]
            )
        block = r.held[a, d - 1] if d else own[a][...]
        placed = dot(r.placing[...], block)
        if a:
            placed = placed * r.slot_weight[...]
        r.stage[a, d] = placed.astype(BF16)
        others = pl.ds(0, (experts - 1) * cap)
        plane[a, d] = copies.start_all(
            [
                (
                    r.stage.at[a, d, span(planes[k][0], cap)],
                    filled[a].at[span(sp, cap), here_of(d)],
                    planes[k],
                )
                for k in range(1, experts)
            ],
            r.stage.at[a, d, others],
            filled[a].at[others, here_of(d)],
            planes[1],
        )
        filled[a][span(sp, cap), here_of(d)] = r.stage[a, d, span(sp, cap), :]

    def pass_on(a, d):
        if (a, d) == relieved:
            line[a, d].wait_recv()
        else:
            plane[a, d].wait_recv()
        here = filled[a].at[:, here_of(d)]
        forward[a, d] = copies.start(here, here, partner)[1]

    def relieve():
        there = filled[relieved[0]].at[:, here_of(0)]
        line[relieved] = copies.start(there, there, lines[relieved[1]])[1]

    def row_loop(body):
        size = total // 2

        def step(i, carry):
            body(span(i, size))
            return carry

        lax.fori_loop(0, 2, step, 0)

    seen = [0, 0]

    def absorb(a, d):
        forward[a, d].wait_recv()
        cols = span(levels[d], pair)
        order = seen[a]
        seen[a] += 1
        if a == 0:
            if order == 0:
                local[2].wait()
                local[3].wait()

            def chunk(rows):
                x = r.slot_rows[rows, cols]
                gate = dot(x, r.wg[cols, :])
                up = dot(x, r.wu[cols, :])
                if order:
                    gate = gate + r.acc_gate[rows, :]
                    up = up + r.acc_up[rows, :]
                if order == deep - 1:
                    sigma = jax.nn.sigmoid(gate)
                    silu = gate * sigma
                    r.hidden[rows, :] = (silu * up).astype(BF16)
                    gate = up * (sigma * (1.0 + gate * (1.0 - sigma)))
                    up = silu
                r.acc_gate[rows, :] = gate
                r.acc_up[rows, :] = up
        else:
            if order == 0:
                local[4].wait()

            def chunk(rows):
                value = dot(r.slot_cot[rows, cols], r.wd[:, cols], NT)
                if order:
                    value = value + r.acc_hidden[rows, :]
                if order < deep - 1:
                    r.acc_hidden[rows, :] = value
                else:
                    r.d_gate[rows, :] = (value * r.acc_gate[rows, :]).astype(BF16)
                    r.d_up[rows, :] = (value * r.acc_up[rows, :]).astype(BF16)

        row_loop(chunk)

    eye = lax.broadcasted_iota(jnp.int32, (channels, channels), 0) == lax.broadcasted_iota(
        jnp.int32, (channels, channels), 1
    )
    place = lax.broadcasted_iota(jnp.int32, (channels, length), 1)

    def to_column(row):
        return jnp.sum(jnp.where(eye, row, 0.0), axis=1, keepdims=True)

    def to_row(column):
        return jnp.sum(jnp.where(eye, column, 0.0), axis=0, keepdims=True)

    def by_head(weights, x, dims):
        return jnp.concatenate(
            [
                dot(weights[h], x[h * HEAD_DIM : (h + 1) * HEAD_DIM, :], dims)
                for h in range(heads)
            ],
            axis=0,
        )

    def prepare_gates():
        for i in range(5, 12):
            local[i].wait()
        conv = r.conv[...].astype(F32)
        prior = r.prior[...].astype(F32)
        recur = jax.nn.sigmoid(by_head(r.wr, r.conv[...], TN))
        gate = jax.nn.sigmoid(by_head(r.wi, r.conv[...], TN))
        rate = -r.rate[pl.ds(tp, 1), :]
        soft = to_column(jnp.maximum(rate, 0.0) + log1p_small(jnp.exp(-jnp.abs(rate))))
        log_decay = -RATE_SCALE * recur * soft + r.jump[...]
        decay = jnp.exp(log_decay)
        norm = jnp.sqrt(-expm1_neg(2.0 * log_decay))
        state = decay * prior + norm * gate * conv
        x = r.pre[...].astype(F32)
        inner = 0.7978845608028654 * (x + 0.044715 * (x * x * x))
        bend = jnp.tanh(inner)
        gelu = 0.5 * x * (1.0 + bend)
        slope = 0.5 * (1.0 + bend) + 0.5 * x * (1.0 - bend * bend) * (
            0.7978845608028654 * (1.0 + 3 * 0.044715 * (x * x))
        )
        r.mixed[...] = (gelu * state).astype(BF16)
        pull = prior * decay - gate * conv * decay * decay / norm
        r.keep[0] = pull * (-RATE_SCALE * soft) * recur * (1.0 - recur)
        r.keep[1] = norm * conv * gate * (1.0 - gate)
        r.keep[2] = norm * gate
        r.keep[3] = slope * state
        r.keep[4] = gelu
        r.keep[5] = decay

    def prepare_scan():
        decay = r.keep[5]
        later = jnp.where(place < length - 1, pltpu.roll(decay, length - 1, 1), 1.0)
        reach, level = 1, 0
        while reach < length:
            inside = place < length - reach
            r.reach[level] = jnp.where(inside, later, 0.0)
            later = later * jnp.where(inside, pltpu.roll(later, length - reach, 1), 1.0)
            reach *= 2
            level += 1
        r.keep[6] = later

    def prepare_taking():
        r.taking[...] = r.placing[...].T

    def scoped(name, fn, *args):
        with jax.named_scope(name):
            fn(*args)

    stages = [(0, 0), (1, 0)] + [(0, d) for d in range(1, deep)]
    stages += [(1, d) for d in range(2, deep)]
    between = {0: prepare_gates, 1: prepare_scan, 2: prepare_taking}
    scoped("issue", issue, *stages[0])
    scoped("issue", issue, *stages[1])
    count = len(stages)
    behind = []
    for i in range(count):
        if i in between:
            scoped("between", between[i])
        if i + 2 < count:
            scoped(f"issue#i={i + 2}", issue, *stages[i + 2])
        if i + 2 == count - 1 - (deep - 1 > 2):
            relieve()
        if i == count - 1:
            scoped("pass_on_relieved", pass_on, *relieved)
            scoped("absorb_relieved", absorb, *stages[i - 1])
            behind = [relieved]
        elif i:
            scoped(f"absorb#i={i - 1}", absorb, *stages[i - 1])
        scoped(f"pass_on#i={i}", pass_on, *stages[i])
    for stage in behind + [stages[-1]]:
        scoped("absorb_last", absorb, *stage)

    fillers = []

    def blocks_of(body, steps, group):
        for start in range(0, steps, group):

            def run(start=start):
                def step(i, carry):
                    body(i)
                    return carry

                lax.fori_loop(start, min(start + group, steps), step, 0)

            fillers.append(run)

    wide = 256

    def gate_block(i):
        rows = r.slot_rows[:, span(i, wide)]
        r.gate_grad[0, span(i, wide), :] = dot(rows, r.d_gate[...], TN).astype(BF16)

    def down_block(i):
        cols = span(i, wide)
        r.down_grad[0, :, cols] = dot(r.hidden[...], r.slot_cot[:, cols], TN).astype(BF16)

    blocks_of(down_block, full // wide, 2)
    blocks_of(gate_block, full // wide, 2)

    def fill(amount):
        for _ in range(amount):
            if fillers:
                scoped("fill", fillers.pop(0))

    halves = max(1, width // 128)
    half = width // halves
    order = list(range(deep - 1, -1, -1))
    core_copy, home_copy, line_copy = {}, {}, {}

    def kept_of(d, start, size):
        room = hidden_units // width
        first = d % room * width + start
        return (r.acc_gate, r.acc_up, r.acc_hidden)[d // room], slice(first, first + size)

    def width_block(d, which):
        def chunk(rows):
            gate, up = r.d_gate[rows, :], r.d_up[rows, :]
            for side in which:
                block = span(levels[d] * CORES + (core if side else 1 - core), width)
                value = dot(gate, r.wg[block, :], NT) + dot(up, r.wu[block, :], NT)
                if side:
                    kept, cols = kept_of(d, 0, width)
                    kept[rows, cols] = value
                else:
                    r.stage[0, d, rows, :] = value.astype(BF16)

        row_loop(chunk)
        if 0 in which:
            core_copy[d] = copies.start(r.stage.at[0, d], r.paired.at[d], partner)[1]

    def ship(d, h):
        if h == 0:
            core_copy[d].wait_recv()
        cols = slice(h * half, (h + 1) * half)
        kept, kept_cols = kept_of(d, h * half, half)
        joint = kept[:, kept_cols] + r.paired[d, :, cols].astype(F32)
        r.stage[1, d, :, cols] = joint.astype(BF16)
        part, others = pl.ds(h * half, half), pl.ds(0, (experts - 1) * cap)
        home_copy[d, h] = copies.start_all(
            [
                (
                    r.stage.at[1, d, span(planes[k][0], cap), part],
                    r.homed.at[h, d, span(sp, cap)],
                    planes[k],
                )
                for k in range(1, experts)
            ],
            r.stage.at[1, d, others, part],
            r.homed.at[h, d, others],
            planes[1],
        )
        r.homed[h, d, span(sp, cap), :] = r.stage[1, d, span(sp, cap), cols]

    def home(d, h):
        home_copy[d, h].wait_recv()
        summed = dot(r.taking[...], r.homed[h, d])
        if d:
            r.line_out[h, d - 1] = summed.astype(BF16)
            line_copy[d, h] = copies.start(
                r.line_out.at[h, d - 1], r.line_in.at[h, d - 1], lines[d]
            )[1]
        else:
            cols = slice(h * half, (h + 1) * half)
            r.sum_own[h] = summed + r.cot[:, cols].astype(F32)

    def spot_of(place_of, h):
        return r.block_grad.at[:, span(place_of * halves + h, half)]

    gathers, shared = {}, {}

    def close_sum(h):
        value = r.sum_own[h]
        for d in order[:-1]:
            line_copy[d, h].wait_recv()
            value = value + r.line_in[h, d - 1].astype(F32)
        r.block_grad[:, span(tp * halves + h, half)] = value.astype(BF16)
        spot = spot_of(tp, h)
        for d in range(1, deep):
            gathers[d, h] = copies.start(
                spot, spot, lines[d], middle if relay and d == 3 else None
            )
        shared[0, h] = copies.start(spot, spot, partner)[1]

    def gather(d, h):
        gathers[d, h][1].wait_recv()
        spot = spot_of(levels[d] * CORES + core, h)
        if relay and d == 2:
            copies.start(spot, spot, lines[1], middle, gathers[3, h][0])
        shared[d, h] = copies.start(spot, spot, partner)[1]

    share = (full // experts) // width
    pieces = {}

    def arrival_of(slot):
        return r.piece_sems.at[slot]

    def use(d, h):
        mix(d, h)
        spread(d, h)

    def mix(d, h):
        shared[d, h].wait_recv()
        value = None if d == 0 and h == 0 else r.d_mixed[...]
        for c in range(CORES):
            cols = span((levels[d] * CORES + c) * halves + h, half)
            part = dot(r.ow[:, cols], r.block_grad[:, cols], NT)
            value = part if value is None else value + part
        r.d_mixed[...] = value

    def spread(d, h):
        for c in range(CORES):
            block = levels[d] * CORES + c
            grads = r.block_grad[:, span(block * halves + h, half)]
            r.product[d, h, c] = dot(r.mixed[...], grads).astype(BF16)
            to, q = lax.div(block, share), lax.rem(block, share)
            copy = pltpu.make_async_remote_copy(
                src_ref=r.product.at[d, h, c],
                dst_ref=r.products.at[sp, q, h],
                send_sem=r.sent_sems.at[(d * halves + h) * CORES + c],
                recv_sem=arrival_of(sp),
                device_id=(to, tp),
                device_id_type=pl.DeviceIdType.MESH,
            )
            pl.when(to != sp)(copy.start)
            copies.sent.append((to != sp, copy))

            @pl.when(to == sp)
            def _():
                r.products[sp, q, h] = r.product[d, h, c]

    with jax.named_scope("settle"):
        copies.finish()
    waiting = [(order[0], h) for h in range(halves)]
    waiting += [(d, h) for h in range(halves) for d in order[1:]]

    def next_home():
        d, h = waiting.pop(0)
        scoped(f"home#h={h}#d={d}", home, d, h)
        return d, h

    scoped("theirs", width_block, order[0], (0,))
    scoped("mine", width_block, order[0], (1,))
    for h in range(halves):
        scoped("ship", ship, order[0], h)
    scoped("pair", width_block, order[1], (0, 1))
    for i in range(2, deep + 1):
        if i < deep:
            scoped("pair", width_block, order[i], (0, 1))
        scoped("ship", ship, order[i - 1], 0)
        if i < deep:
            next_home()
        if i == deep - 1:
            fill(1)
    for h in range(1, halves):
        for d in order[1:]:
            scoped("ship", ship, d, h)
    while waiting:
        d, h = next_home()
        if h and d == order[1]:
            scoped("sum", close_sum, h - 1)
        if h and d == order[-1]:
            for e in range(1, 3):
                scoped("gather", gather, e, h - 1)
        if (d, h) != (order[-1], halves - 1):
            fill(1)
    last = halves - 1
    scoped("sum", close_sum, last)
    for h in range(last):
        for d in range(2):
            scoped("use", use, d, h)
        for d in range(3, deep):
            scoped("gather", gather, d, h)
        scoped("use", use, 2, h)
    fill(1)
    scoped("gather", gather, 1, last)
    for h in range(last):
        for d in range(3, deep):
            scoped("use", use, d, h)
    scoped("use", use, 0, last)
    scoped("gather", gather, 2, last)
    fill(100)
    scoped("mix", mix, 1, last)
    scoped("spread", spread, 1, last)
    for d in range(3, deep):
        scoped("gather", gather, d, last)
        scoped("mix", mix, d - 1, last)
    scoped("mix", mix, deep - 1, last)

    d_mixed = r.d_mixed[...]
    value = d_mixed * r.keep[4]
    reach, level = 1, 0
    while reach < length:
        value = value + r.reach[level] * pltpu.roll(value, length - reach, 1)
        reach *= 2
        level += 1
    decay_first = r.keep[5][:, 0:1]
    r.summary[0, 0:1, :] = to_row(decay_first * r.keep[6][:, 0:1])
    r.summary[0, 1:2, :] = to_row(decay_first * value[:, 0:1])
    ends = copies.start_all(
        [(r.summary.at[0], r.summaries.at[sp], planes[k]) for k in range(1, experts)],
        r.summary.at[pl.ds(0, experts - 1)],
        r.summaries.at[pl.ds(0, experts - 1)],
        planes[1],
    )
    r.summaries[sp] = r.summary[0]
    r.valve[...] = (d_mixed * r.keep[3]).astype(BF16)
    for d in range(2, deep):
        scoped("spread", spread, d, halves - 1)
    with jax.named_scope("settle"):
        copies.finish(len(copies.sent) - (deep - 2) * CORES - 1)
    with jax.named_scope("summaries"):
        ends.wait_recv()
    carried = jnp.zeros((1, channels), F32)
    for later in range(experts - 1, 0, -1):
        longer = r.summaries[later, 1:2, :] + r.summaries[later, 0:1, :] * carried
        carried = jnp.where(later > sp, longer, carried)
    state_grad = value + r.keep[6] * to_column(carried)
    grad_recur = (state_grad * r.keep[0]).astype(BF16)
    grad_input = (state_grad * r.keep[1]).astype(BF16)
    conv_grad = state_grad * r.keep[2]
    conv_grad = conv_grad + by_head(r.wr, grad_recur, NN) + by_head(r.wi, grad_input, NN)
    r.conv_grad[...] = conv_grad.astype(BF16)
    with jax.named_scope("products"):
        for k in range(1, experts):
            spot = r.products.at[planes[k][0]]
            pltpu.make_async_remote_copy(
                src_ref=spot,
                dst_ref=spot,
                send_sem=r.sent_sems.at[0],
                recv_sem=arrival_of(planes[k][0]),
                device_id=planes[k],
                device_id_type=pl.DeviceIdType.MESH,
            ).wait_recv()
    with jax.named_scope("assemble"):
        for q in range(share):
            for h in range(halves):
                value = r.products[0, q, h].astype(F32)
                for e in range(1, experts):
                    value = value + r.products[e, q, h].astype(F32)
                r.out_grad[:, q * width + h * half : q * width + (h + 1) * half] = value
    with jax.named_scope("finish"):
        copies.finish()


def export_kernel(gate, down, out, conv, valve, rows, d_up, *refs):
    outs, (block, sems, up_sems) = refs[:6], refs[6:]
    whole = [
        pltpu.make_async_copy(a, b, sems.at[i])
        for i, (a, b) in enumerate(zip((gate, down, out, conv, valve), outs))
    ]
    for copy in whole:
        copy.start()
    wide = block.shape[1]
    steps = rows.shape[1] // wide
    pieces = []
    for i in range(steps):
        part = pl.ds(i * wide, wide)
        block[i] = dot(rows[:, part], d_up[...], TN).astype(BF16)
        pieces.append(
            pltpu.make_async_copy(block.at[i], outs[5].at[0, part, :], up_sems.at[i])
        )
        pieces[-1].start()
    for copy in whole + pieces:
        copy.wait()


def local(
    cotangent,
    block_input,
    routes,
    route_weights,
    gate_weight,
    up_weight,
    down_weight,
    out_weight,
    conv_out,
    gate_pre,
    prior_states,
    recur_weight,
    input_gate_matrix,
    decay_param,
    decay_jump,
):
    experts, columns = lax.axis_size("sp"), lax.axis_size("tp")
    deep = columns // CORES
    tokens, width = cotangent.shape
    cap = -(-(5 * tokens * TOP_K // (4 * experts)) // 16) * 16
    total = experts * cap
    full = width * columns
    units = gate_weight.shape[2]
    channels, length = conv_out.shape
    heads = channels // HEAD_DIM
    doublings = (length - 1).bit_length()
    halves = max(1, width // 128)
    half = width // halves
    share = (full // experts) // width
    relays = int(deep == 4)
    in_dispatch = 3 * (2 * deep - 1) + 2 * relays
    in_combine = deep + halves * (4 * deep - 2) + 1
    sends = max(in_dispatch, in_combine + halves * relays)
    vmem = pltpu.VMEM
    scratch = dict(
        rows=vmem((tokens, width), BF16),
        cot=vmem((tokens, width), BF16),
        wg=vmem((full, units), BF16),
        wu=vmem((full, units), BF16),
        wd=vmem((units, full), BF16),
        ow=vmem((channels, full), BF16),
        conv=vmem((channels, length), BF16),
        pre=vmem((channels, length), BF16),
        prior=vmem((channels, length), BF16),
        jump=vmem((channels, length), F32),
        wr=vmem((heads, HEAD_DIM, HEAD_DIM), BF16),
        wi=vmem((heads, HEAD_DIM, HEAD_DIM), BF16),
        held=vmem((2, deep - 1, tokens, width), BF16),
        placing=vmem((total, tokens), BF16),
        taking=vmem((tokens, total), BF16),
        slot_weight=vmem((total, 1), F32),
        stage=vmem((2, deep, total, width), BF16),
        slot_cot=vmem((total, full), BF16),
        acc_gate=vmem((total, units), F32),
        acc_up=vmem((total, units), F32),
        acc_hidden=vmem((total, units), F32),
        hidden=vmem((total, units), BF16),
        d_gate=vmem((total, units), BF16),
        paired=vmem((deep, total, width), BF16),
        homed=vmem((halves, deep, total, half), BF16),
        line_out=vmem((halves, deep - 1, tokens, half), BF16),
        line_in=vmem((halves, deep - 1, tokens, half), BF16),
        sum_own=vmem((halves, tokens, half), F32),
        block_grad=vmem((tokens, full), BF16),
        mixed=vmem((channels, length), BF16),
        d_mixed=vmem((channels, length), F32),
        keep=vmem((7, channels, length), F32),
        reach=vmem((doublings, channels, length), F32),
        product=vmem((deep, halves, CORES, channels, half), BF16),
        products=vmem((experts, share, halves, channels, half), BF16),
        summary=vmem((experts - 1, 8, channels), F32),
        summaries=vmem((experts, 8, channels), F32),
        send_sems=pltpu.SemaphoreType.DMA((sends,)),
        recv_sems=pltpu.SemaphoreType.DMA((in_dispatch + in_combine,)),
        local_sems=pltpu.SemaphoreType.DMA((12,)),
        sent_sems=pltpu.SemaphoreType.DMA((deep * halves * CORES,)),
        piece_sems=pltpu.SemaphoreType.DMA((experts,)),
    )
    on_chip = pl.BlockSpec(memory_space=pltpu.VMEM)
    far = pl.BlockSpec(memory_space=pltpu.HBM)
    given = ("routes", "route_w", "rate")

    def in_hbm(x):
        return pltpu.with_memory_space_constraint(x, pltpu.HBM)

    results = pl.pallas_call(
        functools.partial(kernel, INPUTS + OUTPUTS + tuple(scratch), experts, deep, cap),
        out_shape=(
            vmem(gate_weight.shape, BF16),
            vmem(down_weight.shape, BF16),
            vmem((channels, full // experts), F32),
            vmem((channels, length), BF16),
            vmem((channels, length), BF16),
            vmem((total, full), BF16),
            vmem((total, units), BF16),
        ),
        in_specs=[on_chip if name in given else far for name in INPUTS],
        out_specs=(on_chip,) * len(OUTPUTS),
        scratch_shapes=list(scratch.values()),
        compiler_params=pltpu.CompilerParams(
            collective_id=0, has_side_effects=True, vmem_limit_bytes=50 << 20
        ),
    )(
        in_hbm(block_input),
        in_hbm(cotangent),
        jnp.transpose(routes),
        jnp.transpose(route_weights),
        in_hbm(gate_weight),
        in_hbm(up_weight),
        in_hbm(down_weight),
        in_hbm(out_weight),
        in_hbm(conv_out),
        in_hbm(gate_pre),
        in_hbm(prior_states),
        in_hbm(recur_weight),
        in_hbm(input_gate_matrix),
        decay_param.reshape(columns, channels),
        in_hbm(decay_jump),
    )
    wide = 256
    saved = [jax.ShapeDtypeStruct(x.shape, x.dtype) for x in results[:5]]
    gate, down, out, conv, valve, up = pl.pallas_call(
        export_kernel,
        out_shape=saved + [jax.ShapeDtypeStruct(up_weight.shape, BF16)],
        in_specs=[on_chip] * len(results),
        out_specs=[far] * 6,
        scratch_shapes=[
            vmem((full // wide, wide, units), BF16),
            pltpu.SemaphoreType.DMA((5,)),
            pltpu.SemaphoreType.DMA((full // wide,)),
        ],
        compiler_params=pltpu.CompilerParams(vmem_limit_bytes=12 << 20),
    )(*results)
    return gate, up, down, out, conv, valve


def solution(mesh):
    in_specs = (
        P("sp", "tp"),
        P("sp", "tp"),
        P("sp", None),
        P("sp", None),
        P("sp", None, "tp"),
        P("sp", None, "tp"),
        P("sp", "tp", None),
        P("tp", None),
        P("tp", "sp"),
        P("tp", "sp"),
        P("tp", "sp"),
        P(),
        P(),
        P(),
        P("tp", "sp"),
    )
    out_specs = (
        P("sp", None, "tp"),
        P("sp", None, "tp"),
        P("sp", "tp", None),
        P("tp", "sp"),
        P("tp", "sp"),
        P("tp", "sp"),
    )
    return jax.shard_map(local, mesh=mesh, in_specs=in_specs, out_specs=out_specs, check_vma=False)
```
